128 devices in a mesh: kv: 16 (over z, y), tp: 8 (over x, core).
Axes of the slice: x: 4, y: 4, z: 4, core: 2. Of those that a mesh axis runs over, the one named last changes fastest.
Arguments:
- tokens: bfloat16 [256, 4, 2048], P(None, None, ('kv', 'tp')), may hold values from -520 to 520
- input_norm_gain: bfloat16 [2048], replicated, may hold values from 0.099609375 to 1.8984375
- query_weight: bfloat16 [2048, 2048], P(None, 'kv'), may hold values from -0.125 to 0.125
- key_weight: bfloat16 [2048, 2048], P(None, 'kv'), may hold values from -0.125 to 0.125
- value_weight: bfloat16 [2048, 16, 128], P(None, 'kv', 'tp'), may hold values from -1.14904852 to 1.14904852
- output_gate_weight: bfloat16 [2048, 16, 128], P(None, 'kv', 'tp'), may hold values from -0.125 to 0.125
- strength_weight: bfloat16 [2048, 16], P(None, 'kv'), may hold values from -0.125 to 0.125
- decay_weight: bfloat16 [2048, 16], P(None, 'kv'), may hold values from -0.125 to 0.125
- head_decay_rate: float32 [16], P('kv'), may hold values from 0.005 to 1.5
- proposal_log_decay: float32 [256, 4, 16], P(None, None, 'kv'), may hold values from -0.69 to 0
- head_norm_gain: bfloat16 [128], P('tp'), may hold values from 0.099609375 to 1.8984375
- output_weight: bfloat16 [16, 128, 2048], P('kv', 'tp'), may hold values from -1.14904852 to 1.14904852
- output_norm_gain: bfloat16 [2048], P(('kv', 'tp')), may hold values from 0.099609375 to 1.8984375
- state: float32 [256, 16, 128, 128], P(None, 'kv', 'tp'), may hold values from -4.5961941 to 4.5961941
- previous_keys: bfloat16 [256, 4, 2048], P(None, None, 'kv'), may hold values from -6 to 6
- previous_values: bfloat16 [256, 4, 16, 128], P(None, None, 'kv', 'tp'), may hold values from -52 to 52
- previous_log_decay: float32 [256, 4, 16], P(None, None, 'kv'), may hold values from -0.7 to -0.02
- previous_strengths: float32 [256, 4, 16], P(None, None, 'kv'), may hold values from 0.1 to 0.9
- accepted: int32 [256], replicated, may hold values from 0 to 4
- parent: int32 [256, 4], replicated, may hold values from -1 to 2, as said below
Outputs:
- layer_out: bfloat16 [256, 4, 2048], P(None, None, ('kv', 'tp'))
- accepted_state: float32 [256, 16, 128, 128], P(None, 'kv', 'tp')
The draws below stay inside these ranges and needn't reach their ends.
Inputs may be any that keep to these rules, and one draw needn't show every extreme that they name: parent[b, i] is -1 or a proposal index below i; -1 means that proposal i follows the accepted old proposals directly.
All inputs are finite; a program needn't handle non-finite values.
Results may differ from the reference program's by a relative error of at most 0.019.
Values may be sent and summed in bfloat16 or wider, within the bound.
A program may use at most 128 MiB of HBM per device.

```python
import jax
import jax.numpy as jnp
from jax import lax

D = 2048
H = 16
HD = 128
PROP = 4
SEQS = 256


def column_scales(key, count):
    position = jnp.arange(count, dtype=jnp.float32) / max(count - 1, 1)
    spread = jax.random.uniform(key, (count,), jnp.float32)
    return jnp.exp(jnp.log(3.0) * position + jnp.log(3.4) * spread)


def rough_base(key, shape):
    base = jax.random.normal(key, shape, jnp.float32)
    return jnp.clip(base, -5.0, 5.0)


def draw_tokens(key, part):
    subkeys = jax.random.split(jax.random.fold_in(key, 11), 3)
    base = rough_base(subkeys[0], (SEQS, PROP, D))
    rowscale = jnp.exp(jnp.log(10.0) * jax.random.uniform(subkeys[2], (SEQS, PROP, 1), jnp.float32))
    return (base * column_scales(subkeys[1], D)[None, None, :] * rowscale).astype(jnp.bfloat16)


def draw_output_weight(key, part):
    subkeys = jax.random.split(jax.random.fold_in(key, 23), 2)
    base = jax.random.normal(subkeys[0], (H, HD, D), jnp.float32)
    base = jnp.clip(base, -5.0, 5.0)
    scaled = base * (H * HD) ** (-0.5) * column_scales(subkeys[1], D)[None, None, :]
    return scaled.astype(jnp.bfloat16)


def draw_value_weight(key, part):
    subkeys = jax.random.split(jax.random.fold_in(key, 61), 2)
    base = rough_base(subkeys[0], (D, H, HD))
    return (base * D ** (-0.5) * column_scales(subkeys[1], HD)[None, None, :]).astype(jnp.bfloat16)


def draw_state(key, part):
    subkeys = jax.random.split(jax.random.fold_in(key, 67), 2)
    base = rough_base(subkeys[0], (SEQS, H, HD, HD))
    return base * HD ** (-0.5) * column_scales(subkeys[1], HD)[None, None, :, None]


def draw_previous_values(key, part):
    subkeys = jax.random.split(jax.random.fold_in(key, 71), 2)
    base = rough_base(subkeys[0], (SEQS, PROP, H, HD))
    return (base * column_scales(subkeys[1], HD)[None, None, None, :]).astype(jnp.bfloat16)


def draw_head_decay_rate(key, part):
    uniform_part = jax.random.uniform(jax.random.fold_in(key, 31), (H,), jnp.float32)
    lowest = 0.02
    highest = 1.5
    return jnp.exp(jnp.log(lowest) + uniform_part * (jnp.log(highest) - jnp.log(lowest)))


def draw_proposal_log_decay(key, part):
    subkeys = jax.random.split(jax.random.fold_in(key, 41), 2)
    chosen = (jax.random.randint(subkeys[0], (SEQS, PROP, H), 0, 4) == 0).astype(jnp.float32)
    depth = jax.random.uniform(subkeys[1], (SEQS, PROP, H), jnp.float32, 0.22, 0.69)
    return -depth * chosen


def draw_parent(key, part):
    raw_bits = jax.random.randint(jax.random.fold_in(key, 53), (SEQS, PROP), 0, 1 << 20)
    column = jnp.arange(PROP, dtype=jnp.int32)
    return (raw_bits % (column[None, :] + 1) - 1).astype(jnp.int32)


def set_ends(drawn, rng, low, top_value):
    extent = drawn.shape
    spot = [jax.random.randint(jax.random.fold_in(rng, axis), (), 0, extent[axis]) for axis in range(len(extent))]
    drawn = drawn.at[tuple(spot)].set(low)
    longest = extent.index(max(extent))
    spot[longest] = (spot[longest] + 1) % extent[longest]
    return drawn.at[tuple(spot)].set(top_value)


def levels(own_key, shape, shards, smallest, high):
    gain, own = 1.0, jax.random.fold_in(own_key, 6)
    for dim, parts in shards:
        draws = jnp.exp(jax.random.uniform(jax.random.fold_in(own, dim), (parts,), jnp.float32, smallest / len(shards), high / len(shards)))
        gain = gain * jnp.repeat(draws, shape[dim] // parts).reshape([-1 if axis == dim else 1 for axis in range(len(shape))])
    return gain


def normal_values(own_key, extent, scale, most, cuts=(), kind=jnp.bfloat16):
    values = scale * jax.random.normal(own_key, extent, jnp.float32)
    if cuts:
        values = values * levels(own_key, extent, cuts, -0.22, 0.18)
    return jnp.clip(values, -most, most).astype(kind)


def setup_inputs(seed: int = 0) -> dict:
    key_list = jax.random.split(jax.random.key(seed), 21)
    tokens = draw_tokens(jax.random.fold_in(key_list[20], 71), 0)
    input_norm_gain = jnp.clip(1.0 + 0.18 * jax.random.normal(key_list[1], (D,), jnp.float32), 0.099609375, 1.8984375).astype(jnp.bfloat16)
    query_weight = normal_values(key_list[2], (D, H * HD), D ** -0.5, 0.125, ((1, 16),))
    key_weight = normal_values(key_list[3], (D, H * HD), D ** -0.5, 0.125, ((1, 16),))
    value_weight = draw_value_weight(jax.random.fold_in(key_list[20], 71), 0)
    output_gate_weight = normal_values(key_list[5], (D, H, HD), D ** -0.5, 0.125, ((1, 16), (2, 8)))
    strength_weight = normal_values(key_list[6], (D, H), D ** -0.5, 0.125, ((1, 16),))
    decay_weight = normal_values(key_list[7], (D, H), D ** -0.5, 0.125, ((1, 16),))
    head_decay_rate = draw_head_decay_rate(jax.random.fold_in(key_list[20], 71), 0)
    proposal_log_decay = draw_proposal_log_decay(jax.random.fold_in(key_list[20], 71), 0)
    head_norm_gain = jnp.clip(1.0 + 0.18 * jax.random.normal(key_list[10], (HD,), jnp.float32), 0.099609375, 1.8984375).astype(jnp.bfloat16)
    output_weight = draw_output_weight(jax.random.fold_in(key_list[20], 71), 0)
    output_norm_gain = jnp.clip(1.0 + 0.18 * jax.random.normal(key_list[12], (D,), jnp.float32), 0.099609375, 1.8984375).astype(jnp.bfloat16)
    state = draw_state(jax.random.fold_in(key_list[20], 71), 0)
    previous_keys = normal_values(key_list[14], (SEQS, PROP, H * HD), 1.0, 6.0, ((2, 16),))
    previous_values = draw_previous_values(jax.random.fold_in(key_list[20], 71), 0)
    previous_log_decay = jnp.clip(-0.7 + 0.68 * jax.random.uniform(key_list[16], (SEQS, PROP, H), jnp.float32) ** levels(key_list[16], (SEQS, PROP, H), ((2, 16),), -0.2, 0.2), -0.7, -0.02)
    previous_strengths = jnp.clip(0.1 + 0.79999997 * jax.random.uniform(key_list[17], (SEQS, PROP, H), jnp.float32) ** levels(key_list[17], (SEQS, PROP, H), ((2, 16),), -0.2, 0.2), 0.1, 0.9)
    accepted = set_ends(jax.random.randint(key_list[18], (SEQS,), 0, PROP + 1), jax.random.fold_in(key_list[18], 1), 0, PROP).astype(jnp.int32)
    parent = draw_parent(jax.random.fold_in(key_list[20], 71), 0)
    return {"tokens": tokens, "input_norm_gain": input_norm_gain, "query_weight": query_weight, "key_weight": key_weight, "value_weight": value_weight, "output_gate_weight": output_gate_weight, "strength_weight": strength_weight, "decay_weight": decay_weight, "head_decay_rate": head_decay_rate, "proposal_log_decay": proposal_log_decay, "head_norm_gain": head_norm_gain, "output_weight": output_weight, "output_norm_gain": output_norm_gain, "state": state, "previous_keys": previous_keys, "previous_values": previous_values, "previous_log_decay": previous_log_decay, "previous_strengths": previous_strengths, "accepted": accepted, "parent": parent}


epsilon = 1e-06

def unit_rows(matrix):
    return matrix * lax.rsqrt(lax.optimization_barrier(jnp.sum(matrix * matrix, axis=-1, keepdims=True)) + epsilon)

def exact_product(form, left, right):
    return jnp.einsum(form, left, right, precision=lax.Precision.HIGHEST)

def visibility(parent):
    sequence_count, proposal_count = parent.shape
    position = jnp.arange(proposal_count, dtype=jnp.int32)
    parent_hot = (parent[:, :, None] == position[None, None, :]).astype(jnp.float32)
    ancestry = []
    for row_index in range(proposal_count):
        ancestor_row = parent_hot[:, row_index, :]
        if row_index > 0:
            earlier = jnp.stack(ancestry, axis=1)
            ancestor_row = ancestor_row + exact_product('bj,bjk->bk', parent_hot[:, row_index, :row_index], earlier)
        ancestry.append(ancestor_row)
    ancestor = jnp.stack(ancestry, axis=1)
    chain = (position[:, None] > position[None, :]).astype(jnp.float32)
    upper = jnp.concatenate([jnp.broadcast_to(chain, (sequence_count, proposal_count, proposal_count)), jnp.zeros((sequence_count, proposal_count, proposal_count), jnp.float32)], axis=2)
    lower = jnp.concatenate([jnp.ones((sequence_count, proposal_count, proposal_count), jnp.float32), ancestor], axis=2)
    return jnp.concatenate([upper, lower], axis=1)

def split_heads(matrix, sequence_count, proposal_count, number_of_heads):
    return matrix.astype(jnp.float32).reshape(sequence_count, proposal_count, number_of_heads, -1).transpose(0, 2, 1, 3)

def delta_recursion(query_projected, key_projected, value_projected, output_gate_logits, write_strength_logits, decay_logits, decay_speed, proposal_group, head_norm_gain, state, previous_keys, previous_values, previous_log_decay, previous_strengths, accepted, parent, channel_count_total):
    sequence_count, number_of_heads, value_dim, head_dim = state.shape
    proposal_count = parent.shape[1]
    queries = unit_rows(split_heads(query_projected, sequence_count, proposal_count, number_of_heads)) * head_dim ** (-0.5)
    new_keys = unit_rows(split_heads(key_projected, sequence_count, proposal_count, number_of_heads))
    old_keys = unit_rows(split_heads(previous_keys, sequence_count, proposal_count, number_of_heads))
    new_values = split_heads(value_projected, sequence_count, proposal_count, number_of_heads)
    old_values = split_heads(previous_values, sequence_count, proposal_count, number_of_heads)
    zgate = split_heads(output_gate_logits, sequence_count, proposal_count, number_of_heads)
    beta_new = jax.nn.sigmoid(write_strength_logits.reshape(sequence_count, proposal_count, number_of_heads)).transpose(0, 2, 1)
    fresh_decay = (-decay_speed[None, None, :] * jax.nn.softplus(decay_logits.reshape(sequence_count, proposal_count, number_of_heads)) + proposal_group).transpose(0, 2, 1)
    position = jnp.arange(proposal_count, dtype=jnp.int32)
    live = (position[None, :] < accepted[:, None]).astype(jnp.float32)[:, None, :]
    beta_old = previous_strengths.transpose(0, 2, 1) * live
    decay_old = previous_log_decay.transpose(0, 2, 1) * live
    keys_all = jnp.concatenate([old_keys, new_keys], axis=2)
    values_all = jnp.concatenate([old_values, new_values], axis=2)
    beta_all = jnp.concatenate([beta_old, beta_new], axis=2)
    decay_all = jnp.concatenate([decay_old, fresh_decay], axis=2)
    visible = visibility(parent)
    gamma_sum = decay_all + exact_product('bij,bhj->bhi', visible, decay_all)
    gamma_diff = gamma_sum[:, :, :, None] - gamma_sum[:, :, None, :]
    decay_pair = jnp.exp(jnp.minimum(gamma_diff, 0.0)) * visible[:, None]
    coupling = beta_all[..., None] * exact_product('bhid,bhjd->bhij', keys_all, keys_all) * decay_pair
    right_side = jnp.concatenate([beta_all[..., None] * values_all, (beta_all * jnp.exp(gamma_sum))[..., None] * keys_all], axis=-1)
    solved = []
    for row_index in range(2 * proposal_count):
        current = right_side[:, :, row_index]
        if row_index > 0:
            current = current - exact_product('bhj,bhjd->bhd', coupling[:, :, row_index, :row_index], jnp.stack(solved, axis=2))
        solved.append(current)
    solution = jnp.stack(solved, axis=2)
    update = solution[..., :value_dim] - exact_product('bhcd,bhed->bhce', solution[..., value_dim:], state)
    identity = jnp.eye(2 * proposal_count, dtype=jnp.float32)
    seen = visible[:, proposal_count:] + identity[proposal_count:][None]
    reach = jnp.exp(jnp.minimum(gamma_diff[:, :, proposal_count:], 0.0)) * seen[:, None]
    query_key = exact_product('bhid,bhjd->bhij', queries, keys_all) * reach
    readout = exact_product('bhid,bhed->bhie', queries * jnp.exp(gamma_sum[:, :, proposal_count:])[..., None], state)
    readout = readout + exact_product('bhij,bhje->bhie', query_key, update)
    squares = channel_count_total(lax.optimization_barrier(jnp.sum(readout * readout, axis=-1)))
    readout = readout * lax.rsqrt(squares / head_dim + epsilon)[..., None]
    readout = readout * head_norm_gain.astype(jnp.float32) * jax.nn.silu(zgate)
    blended_rows = readout.transpose(0, 2, 1, 3).reshape(sequence_count * proposal_count, number_of_heads * value_dim)
    blended_rows = blended_rows.astype(jnp.bfloat16)
    last_gamma = gamma_sum[:, :, proposal_count - 1:proposal_count]
    key_weighted = old_keys * jnp.exp(last_gamma - gamma_sum[:, :, :proposal_count])[..., None]
    accepted_state = jnp.exp(last_gamma)[..., None] * state + exact_product('bhcd,bhce->bhed', key_weighted, update[:, :, :proposal_count])
    return (blended_rows, accepted_state)

def kept_channel_total(squares):
    return squares

def reference(tokens, input_norm_gain, query_weight, key_weight, value_weight, output_gate_weight, strength_weight, decay_weight, head_decay_rate, proposal_log_decay, head_norm_gain, output_weight, output_norm_gain, state, previous_keys, previous_values, previous_log_decay, previous_strengths, accepted, parent):
    sequence_count, proposal_count, width = tokens.shape
    features = tokens.astype(jnp.float32)
    normed = features * lax.rsqrt(lax.optimization_barrier(jnp.mean(features * features, axis=-1, keepdims=True)) + epsilon)
    normed = (normed * input_norm_gain.astype(jnp.float32)).astype(jnp.bfloat16)
    flat_rows = normed.reshape(sequence_count * proposal_count, width)
    query_projected = jnp.dot(flat_rows, query_weight, preferred_element_type=jnp.float32).astype(jnp.bfloat16)
    key_projected = jnp.dot(flat_rows, key_weight, preferred_element_type=jnp.float32).astype(jnp.bfloat16)
    value_projected = jnp.dot(flat_rows, value_weight.reshape(width, -1), preferred_element_type=jnp.float32).astype(jnp.bfloat16)
    output_gate_logits = jnp.dot(flat_rows, output_gate_weight.reshape(width, -1), preferred_element_type=jnp.float32).astype(jnp.bfloat16)
    write_strength_logits = jnp.dot(flat_rows, strength_weight, preferred_element_type=jnp.float32)
    decay_logits = jnp.dot(flat_rows, decay_weight, preferred_element_type=jnp.float32)
    blended_rows, accepted_state = delta_recursion(query_projected, key_projected, value_projected, output_gate_logits, write_strength_logits, decay_logits, head_decay_rate, proposal_log_decay, head_norm_gain, state, previous_keys, previous_values, previous_log_decay, previous_strengths, accepted, parent, kept_channel_total)
    combined = jnp.dot(blended_rows, output_weight.reshape(-1, width), preferred_element_type=jnp.float32)
    combined = combined * lax.rsqrt(lax.optimization_barrier(jnp.mean(combined * combined, axis=-1, keepdims=True)) + epsilon)
    layer_out = (combined * output_norm_gain.astype(jnp.float32)).astype(jnp.bfloat16).reshape(sequence_count, proposal_count, width)
    return (layer_out, accepted_state)
```

```python
import functools

import jax
import jax.numpy as jnp
from jax import lax
from jax.experimental import pallas as pl
from jax.experimental.pallas import tpu as pltpu
from jax.sharding import PartitionSpec as P

EPS = 1e-06
F32 = jnp.float32
BF16 = jnp.bfloat16
MESH = pl.DeviceIdType.MESH
NT = (((1,), (1,)), ((), ()))
NN = (((1,), (0,)), ((), ()))
TN = (((0,), (0,)), ((), ()))


def dot(a, b, dims=NN):
    return lax.dot_general(a, b, dims, preferred_element_type=F32)


def iota(shape, dim):
    return lax.broadcasted_iota(jnp.int32, shape, dim)


def roll(x, shift):
    return x if shift % 128 == 0 else pltpu.roll(x, shift % 128, 1)


def row_to_column(row):
    n = row.shape[1]
    square = jnp.broadcast_to(row, (n, n))
    return jnp.sum(jnp.where(iota((n, n), 0) == iota((n, n), 1), square, 0.0), axis=1, keepdims=True)


def ungroup(parts, j):
    chunk = iota(parts[0].shape, 1) // 32
    halves = []
    for h in range(2):
        total = None
        for m in range(4):
            x = roll(parts[h * 4 + m], (m - j) * 32)
            total = x if total is None else jnp.where(chunk == m, x, total)
        halves.append(total)
    return jnp.concatenate(halves, axis=1)


def regroup(rows, g):
    h, m = divmod(g, 4)
    total = None
    for j in range(4):
        x = roll(rows[j][:, h * 128 : h * 128 + 128], (j - m) * 32)
        total = x if total is None else jnp.where(iota(x.shape, 1) // 32 == j, x, total)
    return total


def pick_rows(product):
    lanes = product.shape[1]
    cube = product.reshape(32, 16, lanes)
    keep = iota(cube.shape, 0) == iota(cube.shape, 2) % 32
    return jnp.sum(jnp.where(keep, cube, 0.0), axis=0)


def pick_pairs(product):
    n, lanes = product.shape[0] // 32, product.shape[1]
    cube = product.reshape(n, 32, lanes)
    keep = iota(cube.shape, 1) == iota(cube.shape, 2) % 32
    return jnp.sum(jnp.where(keep, cube, 0.0), axis=1)


def sum_of(terms):
    return functools.reduce(lambda a, b: a + b, terms)


def old_part(state, keys, old_values, log_decay, strengths, accepted, store):
    source, target = iota((128, 128), 1), iota((128, 128), 0)
    order = (source == (target % 32) * 4 + target // 32).astype(BF16)
    grouped, reads, grams = [], [], []
    for g in range(8):
        kg = dot(order, keys(g)).astype(BF16)
        grouped.append(kg)
        reads.append(pick_rows(dot(state(g).astype(BF16), kg, NT)))
        grams.append(pick_pairs(dot(kg, kg, NT)))
    gram = [ungroup(grams, j) for j in range(4)]
    read = [ungroup(reads, j) for j in range(4)]
    inv = [lax.rsqrt(gram[j][j : j + 1] + EPS) for j in range(4)]
    gam, beta = [], []
    for j in range(4):
        live = (j < accepted).astype(F32)
        g_j = log_decay[j] * live
        gam.append(g_j if j == 0 else gam[-1] + g_j)
        beta.append(strengths[j] * live)
    update = []
    for i in range(4):
        u = beta[i] * (old_values[i] - (jnp.exp(gam[i]) * inv[i]) * read[i])
        for j in range(i):
            a = beta[i] * (gram[j][i : i + 1] * (inv[i] * inv[j])) * jnp.exp(gam[i] - gam[j])
            u = u - a * update[j]
        update.append(u)
    weighted = [update[j] * (jnp.exp(gam[3] - gam[j]) * inv[j]) for j in range(4)]
    kept = jnp.exp(gam[3])
    columns = [jnp.broadcast_to(row_to_column(kept[:, h * 128 : h * 128 + 128]), (128, 128)) for h in range(2)]
    for g in range(8):
        wg = regroup(weighted, g)
        cube = (32, 16, 128)
        keep = iota(cube, 0) == iota(cube, 2) % 32
        block = jnp.where(keep, jnp.broadcast_to(wg[None], cube), 0.0).reshape(512, 128).astype(BF16)
        h, m = divmod(g, 4)
        scale = jnp.broadcast_to(columns[h][m * 32 : m * 32 + 32][:, None, :], cube).reshape(512, 128)
        store(g, scale * state(g) + dot(block, grouped[g]))


def new_part(accepted_state, query_key, values, beta_pre, decay_pre, rate, proposal, parent):
    reads, grams = [], []
    for g in range(8):
        qk = query_key(g)
        reads.append(pick_rows(dot(accepted_state(g), qk, NT)))
        grams.append(pick_pairs(dot(qk, qk, NT)))
    left = [r[:, :128] for r in reads], [r[:, 128:] for r in reads]
    aq = [ungroup(left[0], j) for j in range(4)]
    ak = [ungroup(left[1], j) for j in range(4)]
    gq = [ungroup([r[:, :128] for r in grams], j) for j in range(4)]
    gk = [ungroup([r[:, 128:] for r in grams], j) for j in range(4)]
    inv_q = [lax.rsqrt(gq[j][j : j + 1] + EPS) * (128.0**-0.5) for j in range(4)]
    inv_k = [lax.rsqrt(gk[j][4 + j : 5 + j] + EPS) for j in range(4)]
    ancestors = []
    for i in range(4):
        row = {j: (parent[i] == j).astype(F32) for j in range(i)}
        row = {j: row[j] + sum_of([jnp.zeros_like(row[j])] + [row[m] * ancestors[m][j] for m in range(j + 1, i)]) for j in range(i)}
        ancestors.append(row)
    beta, g_new, gam = [], [], []
    for i in range(4):
        x = decay_pre[i]
        softplus = jnp.maximum(x, 0.0) + jnp.log1p(jnp.exp(-jnp.abs(x)))
        g_new.append(-rate * softplus + proposal[i])
        beta.append(jax.nn.sigmoid(beta_pre[i]))
        gam.append(sum_of([g_new[i]] + [ancestors[i][j] * g_new[j] for j in range(i)]))
    outputs, update = [], []
    for i in range(4):
        grow = jnp.exp(gam[i])
        u = beta[i] * (values[i] - (grow * inv_k[i]) * ak[i])
        o = (grow * inv_q[i]) * aq[i]
        for j in range(i):
            reach = jnp.exp(jnp.minimum(gam[i] - gam[j], 0.0)) * ancestors[i][j] * inv_k[j]
            u = u - (beta[i] * inv_k[i] * gk[j][4 + i : 5 + i] * reach) * update[j]
            o = o + (inv_q[i] * gk[j][i : i + 1] * reach) * update[j]
        update.append(u)
        o = o + (inv_q[i] * gk[i][i : i + 1] * inv_k[i]) * u
        outputs.append(o)
    return outputs


def kernel(
    tp_n, kv_n,
    xt_ref, gain_ref, wq_ref, wk_ref, wv_ref, wz_ref, ws_ref, wd_ref, rate_ref, prop_ref, hgain_ref, wo_ref, ogain_ref,
    state_ref, keys_ref, oldv_ref, logd_ref, strength_ref, accepted_ref, parent_ref,
    out_ref, acc_ref,
    xall, wvz, woall, gaincol, xnorm, qkall, vzall, sdall, abf, ssq1, onorm, oall, part, racc, comb, ssq2, ssq3,
    sa, ra, sb, rb, sv, rv, sz, rz, so, ro, sq, rq, svz, rvz, ssd, rsd, sd1, rd1, se, re, sf, rf, sg, rg, sh, rh,
):
    kv, tp = lax.axis_index("kv"), lax.axis_index("tp")

    def of_tp(d):
        return lax.rem(tp + d, tp_n)

    def of_kv(d):
        return lax.rem(kv + d, kv_n)

    def copy_tp(src, dst, send, recv, d, other=None):
        return pltpu.make_async_remote_copy(
            src_ref=src, dst_ref=dst, send_sem=send.at[d], recv_sem=recv.at[d], device_id=(kv, of_tp(d)), device_id_type=MESH
        )

    def copy_kv(src, dst, send, recv, d):
        return pltpu.make_async_remote_copy(
            src_ref=src, dst_ref=dst, send_sem=send.at[d], recv_sem=recv.at[d], device_id=(of_kv(d), tp), device_id_type=MESH
        )

    barrier = pltpu.get_barrier_semaphore()
    for d in range(1, tp_n):
        pl.semaphore_signal(barrier, inc=1, device_id=(kv, of_tp(d)), device_id_type=MESH)
    for d in range(1, kv_n):
        pl.semaphore_signal(barrier, inc=1, device_id=(of_kv(d), tp), device_id_type=MESH)
    pl.semaphore_wait(barrier, tp_n - 1 + kv_n - 1)

    def tile(t):
        return t // 2, pl.ds(pl.multiple_of((t % 2) * 128, 128), 128)

    own_rows = pl.ds(pl.multiple_of((kv * tp_n + tp) * 16, 16), 16)
    pending = []
    stage_a = []
    for d in range(1, tp_n):
        p, lanes = tile(of_tp(d))
        stage_a.append(copy_tp(xt_ref.at[p, :, lanes], xall.at[own_rows], sa, ra, d))
    for c in stage_a:
        c.start()
    p, lanes = tile(tp)
    xall[own_rows, :] = xt_ref[p, :, lanes]

    stage_w = []
    for d in range(1, kv_n):
        cols = pl.ds(pl.multiple_of(of_kv(d) * 128, 128), 128)
        stage_w.append(copy_kv(wo_ref.at[:, cols], woall.at[kv], so, ro, d))
    for d in range(1, tp_n):
        stage_w.append(copy_tp(wv_ref, wvz.at[tp, 0], sv, rv, d))
        stage_w.append(copy_tp(wz_ref, wvz.at[tp, 1], sz, rz, d))
    for c in stage_w:
        c.start()
    woall[kv] = wo_ref[:, pl.ds(pl.multiple_of(kv * 128, 128), 128)]
    wvz[tp, 0] = wv_ref[...]
    wvz[tp, 1] = wz_ref[...]
    for n in range(16):
        column = row_to_column(gain_ref[:, n * 128 : n * 128 + 128].astype(F32))
        gaincol[n * 128 : n * 128 + 128, :] = jnp.broadcast_to(column, (128, 128))

    for c in stage_a:
        c.wait_recv()
    block = pl.ds(pl.multiple_of(kv * 128, 128), 128)
    stage_b = [copy_kv(xall.at[block], xall.at[block], sb, rb, d) for d in range(1, kv_n)]
    for c in stage_b:
        c.start()

    def store(g, value):
        acc_ref[g * 512 : g * 512 + 512, :] = value
        abf[g * 512 : g * 512 + 512, :] = value.astype(BF16)

    old_part(
        lambda g: state_ref[g * 512 : g * 512 + 512, :],
        lambda g: keys_ref[g * 128 : g * 128 + 128, :],
        [oldv_ref[j].astype(F32) for j in range(4)],
        [logd_ref[j] for j in range(4)],
        [strength_ref[j] for j in range(4)],
        accepted_ref[...],
        store,
    )

    for c in stage_b:
        c.wait_recv()
    squares = sum_of([jnp.sum(jnp.square(xall[n * 128 : n * 128 + 128, :].astype(F32)), axis=0, keepdims=True) for n in range(16)])
    scale = lax.rsqrt(squares / 2048.0 + EPS)
    for n in range(16):
        rows = slice(n * 128, n * 128 + 128)
        xnorm[rows, :] = (xall[rows, :].astype(F32) * scale * gaincol[rows, :]).astype(BF16)
    x = xnorm[...]
    qkall[tp, :, 0:128] = dot(x, wq_ref[...], TN).astype(BF16)
    qkall[tp, :, 128:256] = dot(x, wk_ref[...], TN).astype(BF16)
    first = iota((16, 2048), 0) == 0
    wsd = jnp.where(first, jnp.broadcast_to(ws_ref[...].astype(F32), (16, 2048)), jnp.broadcast_to(wd_ref[...].astype(F32), (16, 2048)))
    sdall[tp] = dot(wsd.astype(BF16), x)[0:8]
    stage_c = []
    for d in range(1, tp_n):
        stage_c.append(copy_tp(qkall.at[tp], qkall.at[tp], sq, rq, d))
        stage_c.append(copy_tp(sdall.at[tp], sdall.at[tp], ssd, rsd, d))
    for c in stage_c:
        c.start()
    for c in stage_w:
        c.wait_recv()
    vz = dot(wvz[...].reshape(256, 2048), x).astype(BF16)
    part_vz = vz.reshape(8, 32, 128)
    for t in range(8):
        xvz = part_vz[t]
        part[t, 0:2] = xvz.reshape(2, 16, 128)
    stage_v = []
    for d in range(1, tp_n):
        stage_v.append(copy_tp(part.at[of_tp(d), pl.ds(0, 2)], vzall.at[tp], svz, rvz, d))
    for c in stage_v:
        c.start()
    vzall[tp] = part[tp, 0:2]
    for c in stage_c + stage_v:
        c.wait_recv()

    def query_key(g):
        h, m = divmod(g, 4)
        pieces = [qkall[p * 2 + h, m * 32 : m * 32 + 32, s * 128 : s * 128 + 128] for s in range(2) for p in range(4)]
        return jnp.concatenate(pieces, axis=0)

    def both(f):
        return [jnp.concatenate([f(p * 2), f(p * 2 + 1)], axis=1) for p in range(4)]

    outputs = new_part(
        lambda g: abf[g * 512 : g * 512 + 512, :],
        query_key,
        both(lambda t: vzall[t, 0].astype(F32)),
        both(lambda t: sdall[t, 0:1, :]),
        both(lambda t: sdall[t, 1:2, :]),
        rate_ref[0],
        [prop_ref[j] for j in range(4)],
        [parent_ref[j : j + 1, :] for j in range(4)],
    )
    zgate = both(lambda t: vzall[t, 1].astype(F32))
    hgain = jnp.broadcast_to(row_to_column(hgain_ref[...].astype(F32)), (16, 256))
    sums = [jnp.sum(jnp.square(o), axis=0, keepdims=True) for o in outputs]
    for t in range(8):
        ssq1[tp, t : t + 1, :] = sums[t // 2][:, (t % 2) * 128 : (t % 2) * 128 + 128]
    stage_d = [copy_tp(ssq1.at[tp], ssq1.at[tp], sd1, rd1, d) for d in range(1, tp_n)]
    for c in stage_d:
        c.start()
    gated = [o * hgain * (z * jax.nn.sigmoid(z)) for o, z in zip(outputs, zgate)]
    for c in stage_d:
        c.wait_recv()
    scale = lax.rsqrt(jnp.sum(ssq1[...], axis=0) / 128.0 + EPS)
    for t in range(8):
        y = gated[t // 2][:, (t % 2) * 128 : (t % 2) * 128 + 128]
        onorm[t] = (y * scale[t : t + 1, :]).astype(BF16)
    stage_e = [copy_kv(onorm, oall.at[:, kv], se, re, d) for d in range(1, kv_n)]
    for c in stage_e:
        c.start()
    oall[:, kv] = onorm[...]
    weight = woall[...].reshape(256, 128)
    for c in stage_c + stage_v + stage_a + stage_b + stage_w + stage_d:
        c.wait_send()
    for c in stage_e:
        c.wait_recv()
    for t in range(8):
        product = dot(weight, oall[t].reshape(256, 128), TN)
        part[:, t] = product.astype(BF16).reshape(8, 16, 128)
    stage_f = [copy_tp(part.at[of_tp(d)], racc.at[tp], sf, rf, d) for d in range(1, tp_n)]
    for c in stage_f:
        c.start()
    racc[tp] = part[tp]
    for c in stage_f:
        c.wait_recv()
    for t in range(8):
        total = sum_of([racc[s, t].astype(F32) for s in range(8)])
        comb[t] = total
        ssq2[tp, t : t + 1, :] = jnp.sum(jnp.square(total), axis=0, keepdims=True)
    stage_g = [copy_tp(ssq2.at[tp], ssq2.at[tp], sg, rg, d) for d in range(1, tp_n)]
    for c in stage_g:
        c.start()
    for c in stage_g:
        c.wait_recv()
    ssq3[kv] = jnp.sum(ssq2[...], axis=0)
    stage_h = [copy_kv(ssq3.at[kv], ssq3.at[kv], sh, rh, d) for d in range(1, kv_n)]
    for c in stage_h:
        c.start()
    ogain = jnp.broadcast_to(row_to_column(ogain_ref[...].astype(F32)), (16, 128))
    for c in stage_h:
        c.wait_recv()
    scale = lax.rsqrt(jnp.sum(ssq3[...], axis=0) / 2048.0 + EPS)
    for t in range(8):
        out_ref[t // 2, :, (t % 2) * 128 : (t % 2) * 128 + 128] = (comb[t] * scale[t : t + 1, :] * ogain).astype(BF16)
    for c in stage_e + stage_f + stage_g + stage_h:
        c.wait_send()


def on_device(
    tokens, input_norm_gain, query_weight, key_weight, value_weight, output_gate_weight, strength_weight, decay_weight,
    head_decay_rate, proposal_log_decay, head_norm_gain, output_weight, output_norm_gain, state, previous_keys,
    previous_values, previous_log_decay, previous_strengths, accepted, parent,
):
    tp_n, kv_n = lax.axis_size("tp"), lax.axis_size("kv")
    args = [
        tokens.transpose(1, 2, 0),
        input_norm_gain.reshape(1, -1),
        query_weight,
        key_weight,
        value_weight.transpose(1, 2, 0).reshape(16, 2048),
        output_gate_weight.transpose(1, 2, 0).reshape(16, 2048),
        strength_weight.transpose(1, 0),
        decay_weight.transpose(1, 0),
        head_decay_rate,
        proposal_log_decay.transpose(1, 2, 0),
        head_norm_gain.reshape(1, 16),
        output_weight.reshape(16, 2048),
        output_norm_gain.reshape(1, 16),
        state.reshape(4096, 128),
        previous_keys.reshape(1024, 128),
        previous_values.transpose(1, 2, 3, 0).reshape(4, 16, 256),
        previous_log_decay.transpose(1, 2, 0),
        previous_strengths.transpose(1, 2, 0),
        accepted.reshape(1, 256),
        parent.transpose(1, 0),
    ]
    vmem = pl.BlockSpec(memory_space=pltpu.VMEM)
    specs = [vmem] * len(args)
    specs[8] = pl.BlockSpec(memory_space=pltpu.SMEM)

    def sems(n):
        return [pltpu.SemaphoreType.DMA((n,)), pltpu.SemaphoreType.DMA((n,))]

    out, acc = pl.pallas_call(
        functools.partial(kernel, tp_n, kv_n),
        out_shape=(jax.ShapeDtypeStruct((4, 16, 256), BF16), jax.ShapeDtypeStruct((4096, 128), F32)),
        in_specs=specs,
        out_specs=(vmem, vmem),
        scratch_shapes=[
            pltpu.VMEM((2048, 128), BF16),
            pltpu.VMEM((8, 2, 16, 2048), BF16),
            pltpu.VMEM((16, 16, 128), BF16),
            pltpu.VMEM((2048, 128), F32),
            pltpu.VMEM((2048, 128), BF16),
            pltpu.VMEM((8, 128, 256), BF16),
            pltpu.VMEM((8, 2, 16, 128), BF16),
            pltpu.VMEM((8, 8, 128), F32),
            pltpu.VMEM((4096, 128), BF16),
            pltpu.VMEM((8, 8, 128), F32),
            pltpu.VMEM((8, 16, 128), BF16),
            pltpu.VMEM((8, 16, 16, 128), BF16),
            pltpu.VMEM((8, 8, 16, 128), BF16),
            pltpu.VMEM((8, 8, 16, 128), BF16),
            pltpu.VMEM((8, 16, 128), F32),
            pltpu.VMEM((8, 8, 128), F32),
            pltpu.VMEM((16, 8, 128), F32),
            *sems(8), *sems(16), *sems(8), *sems(8), *sems(16), *sems(8), *sems(8), *sems(8), *sems(8), *sems(16), *sems(8),
            *sems(8), *sems(16),
        ],
        compiler_params=pltpu.CompilerParams(collective_id=0, has_side_effects=True, vmem_limit_bytes=48 << 20),
    )(*args)
    return out.transpose(2, 0, 1), acc.reshape(256, 1, 16, 128)


def solution(mesh):
    placed = (
        P(None, None, ("kv", "tp")),
        P(),
        P(None, "kv"),
        P(None, "kv"),
        P(None, "kv", "tp"),
        P(None, "kv", "tp"),
        P(None, "kv"),
        P(None, "kv"),
        P("kv"),
        P(None, None, "kv"),
        P("tp"),
        P("kv", "tp", None),
        P(("kv", "tp")),
        P(None, "kv", "tp", None),
        P(None, None, "kv"),
        P(None, None, "kv", "tp"),
        P(None, None, "kv"),
        P(None, None, "kv"),
        P(),
        P(),
    )
    return jax.shard_map(
        on_device,
        mesh=mesh,
        in_specs=placed,
        out_specs=(P(None, None, ("kv", "tp")), P(None, "kv", "tp", None)),
        check_vma=False,
    )
```

```python
import functools

import jax
import jax.numpy as jnp
from jax import lax
from jax.experimental import pallas as pl
from jax.experimental.pallas import tpu as pltpu
from jax.sharding import PartitionSpec as P

EPS = 1e-06
INPUTS = 20
F32 = jnp.float32
BF16 = jnp.bfloat16
MESH = pl.DeviceIdType.MESH
NT = (((1,), (1,)), ((), ()))
NN = (((1,), (0,)), ((), ()))
TN = (((0,), (0,)), ((), ()))


def dot(a, b, dims=NN):
    return lax.dot_general(a, b, dims, preferred_element_type=F32)


def iota(shape, dim):
    return lax.broadcasted_iota(jnp.int32, shape, dim)


def roll(x, shift):
    return x if shift % 128 == 0 else pltpu.roll(x, shift % 128, 1)


def row_to_column(row):
    n = row.shape[1]
    square = jnp.broadcast_to(row, (n, n))
    return jnp.sum(jnp.where(iota((n, n), 0) == iota((n, n), 1), square, 0.0), axis=1, keepdims=True)


def ungroup(parts, j):
    chunk = iota(parts[0].shape, 1) // 32
    halves = []
    for h in range(2):
        total = None
        for m in range(4):
            x = roll(parts[h * 4 + m], (m - j) * 32)
            total = x if total is None else jnp.where(chunk == m, x, total)
        halves.append(total)
    return jnp.concatenate(halves, axis=1)


def regroup(rows, g):
    h, m = divmod(g, 4)
    total = None
    for j in range(4):
        x = roll(rows[j][:, h * 128 : h * 128 + 128], (j - m) * 32)
        total = x if total is None else jnp.where(iota(x.shape, 1) // 32 == j, x, total)
    return total


def pick_rows(product):
    lanes = product.shape[1]
    cube = product.reshape(32, 16, lanes)
    keep = iota(cube.shape, 0) == iota(cube.shape, 2) % 32
    return jnp.sum(jnp.where(keep, cube, 0.0), axis=0)


def pick_pairs(product):
    n, lanes = product.shape[0] // 32, product.shape[1]
    cube = product.reshape(n, 32, lanes)
    keep = iota(cube.shape, 1) == iota(cube.shape, 2) % 32
    return jnp.sum(jnp.where(keep, cube, 0.0), axis=1)


def sum_of(terms):
    return functools.reduce(lambda a, b: a + b, terms)


def old_part(state, keys, old_values, log_decay, strengths, accepted, store):
    source, target = iota((128, 128), 1), iota((128, 128), 0)
    order = (source == (target % 32) * 4 + target // 32).astype(BF16)
    grouped, reads, grams = [], [], []
    for g in range(8):
        kg = dot(order, keys(g)).astype(BF16)
        grouped.append(kg)
        reads.append(pick_rows(dot(state(g).astype(BF16), kg, NT)))
        grams.append(pick_pairs(dot(kg, kg, NT)))
    gram = [ungroup(grams, j) for j in range(4)]
    read = [ungroup(reads, j) for j in range(4)]
    inv = [lax.rsqrt(gram[j][j : j + 1] + EPS) for j in range(4)]
    gam, beta = [], []
    for j in range(4):
        live = (j < accepted).astype(F32)
        g_j = log_decay[j] * live
        gam.append(g_j if j == 0 else gam[-1] + g_j)
        beta.append(strengths[j] * live)
    update = []
    for i in range(4):
        u = beta[i] * (old_values[i] - (jnp.exp(gam[i]) * inv[i]) * read[i])
        for j in range(i):
            a = beta[i] * (gram[j][i : i + 1] * (inv[i] * inv[j])) * jnp.exp(gam[i] - gam[j])
            u = u - a * update[j]
        update.append(u)
    weighted = [update[j] * (jnp.exp(gam[3] - gam[j]) * inv[j]) for j in range(4)]
    kept = jnp.exp(gam[3])
    columns = [jnp.broadcast_to(row_to_column(kept[:, h * 128 : h * 128 + 128]), (128, 128)) for h in range(2)]
    for g in range(8):
        wg = regroup(weighted, g)
        cube = (32, 16, 128)
        keep = iota(cube, 0) == iota(cube, 2) % 32
        block = jnp.where(keep, jnp.broadcast_to(wg[None], cube), 0.0).reshape(512, 128).astype(BF16)
        h, m = divmod(g, 4)
        scale = jnp.broadcast_to(columns[h][m * 32 : m * 32 + 32][:, None, :], cube).reshape(512, 128)
        store(g, scale * state(g) + dot(block, grouped[g]))


def new_part(accepted_state, query_key, values, beta_pre, decay_pre, rate, proposal, parent):
    reads, grams = [], []
    for g in range(8):
        qk = query_key(g)
        reads.append(pick_rows(dot(accepted_state(g), qk, NT)))
        grams.append(pick_pairs(dot(qk, qk, NT)))
    left = [r[:, :128] for r in reads], [r[:, 128:] for r in reads]
    aq = [ungroup(left[0], j) for j in range(4)]
    ak = [ungroup(left[1], j) for j in range(4)]
    gq = [ungroup([r[:, :128] for r in grams], j) for j in range(4)]
    gk = [ungroup([r[:, 128:] for r in grams], j) for j in range(4)]
    inv_q = [lax.rsqrt(gq[j][j : j + 1] + EPS) * (128.0**-0.5) for j in range(4)]
    inv_k = [lax.rsqrt(gk[j][4 + j : 5 + j] + EPS) for j in range(4)]
    ancestors = []
    for i in range(4):
        row = {j: (parent[i] == j).astype(F32) for j in range(i)}
        row = {j: row[j] + sum_of([jnp.zeros_like(row[j])] + [row[m] * ancestors[m][j] for m in range(j + 1, i)]) for j in range(i)}
        ancestors.append(row)
    beta, g_new, gam = [], [], []
    for i in range(4):
        x = decay_pre[i]
        softplus = jnp.maximum(x, 0.0) + jnp.log1p(jnp.exp(-jnp.abs(x)))
        g_new.append(-rate * softplus + proposal[i])
        beta.append(jax.nn.sigmoid(beta_pre[i]))
        gam.append(sum_of([g_new[i]] + [ancestors[i][j] * g_new[j] for j in range(i)]))
    outputs, update = [], []
    for i in range(4):
        grow = jnp.exp(gam[i])
        u = beta[i] * (values[i] - (grow * inv_k[i]) * ak[i])
        o = (grow * inv_q[i]) * aq[i]
        for j in range(i):
            reach = jnp.exp(jnp.minimum(gam[i] - gam[j], 0.0)) * ancestors[i][j] * inv_k[j]
            u = u - (beta[i] * inv_k[i] * gk[j][4 + i : 5 + i] * reach) * update[j]
            o = o + (inv_q[i] * gk[j][i : i + 1] * reach) * update[j]
        update.append(u)
        o = o + (inv_q[i] * gk[i][i : i + 1] * inv_k[i]) * u
        outputs.append(o)
    return outputs


def kernel(
    tp_n, kv_n, *refs,
):
    sources, (out_ref, acc_ref), held, scratch = refs[:INPUTS], refs[INPUTS : INPUTS + 2], refs[INPUTS + 2 : 2 * INPUTS + 2], refs[2 * INPUTS + 2 :]
    run(tp_n, kv_n, sources, out_ref, acc_ref, *held, *scratch)


def run(
    tp_n, kv_n, sources, out_ref, acc_ref,
    xt_ref, wv_ref, wz_ref, wo_ref, gain_ref, keys_ref, state_ref, oldv_ref, logd_ref, strength_ref, accepted_ref,
    wq_ref, wk_ref, ws_ref, wd_ref, rate_ref, prop_ref, parent_ref, hgain_ref, ogain_ref,
    load_sems, accv, acc_sems,
    xall, wvz, woall, gaincol, xnorm, qkall, vzs, vzall, sdall, abf, ybuf, yall, sqs, sqall, csend, call, sqf,
    st, rt, sv, rv, swm, rwm, sq, rq, ssd, rsd, sqm, rqm, sdm, rdm, svz, rvz, so, ro, som, rom, se, re, ses, res, sf, rf, sh, rh,
):
    held = (
        xt_ref, wv_ref, wz_ref, wo_ref, gain_ref, keys_ref, state_ref, oldv_ref, logd_ref, strength_ref, accepted_ref,
        wq_ref, wk_ref, ws_ref, wd_ref, rate_ref, prop_ref, parent_ref, hgain_ref, ogain_ref,
    )
    loads = [pltpu.make_async_copy(src, dst, load_sems.at[n]) for n, (src, dst) in enumerate(zip(sources, held))]
    for c in loads:
        c.start()
    kv, tp = lax.axis_index("kv"), lax.axis_index("tp")
    chip, core = tp // 2, lax.rem(tp, 2)
    mate = tp + 1 - 2 * core
    own = kv * tp_n + tp
    everyone = [(a, b) for a in range(kv_n) for b in range(tp_n) if a or b]

    def device(a, b):
        return lax.rem(kv + a, kv_n), lax.rem(tp + b, tp_n)

    def send(src, dst, send_sem, recv_sem, target):
        c = remote(src, dst, send_sem, recv_sem, target)
        c.start()
        return c

    def remote(src, dst, send_sem, recv_sem, target):
        return pltpu.make_async_remote_copy(
            src_ref=src, dst_ref=dst, send_sem=send_sem, recv_sem=recv_sem, device_id=target, device_id_type=MESH
        )

    def total(ref, send_sem, recv_sem):
        return remote(ref, ref, send_sem, recv_sem, (kv, mate))

    def along_chips(d):
        return lax.rem(chip + d, 4) * 2 + core

    def lanes_of(t):
        return pl.ds(pl.multiple_of(lax.rem(t, 2) * 128, 128), 128)

    barrier = pltpu.get_barrier_semaphore()
    for a, b in everyone:
        pl.semaphore_signal(barrier, inc=1, device_id=device(a, b), device_id_type=MESH)
    for c in loads[:5]:
        c.wait()
    with jax.named_scope("barrier"):
        pl.semaphore_wait(barrier, kv_n * tp_n - 1)

    with jax.named_scope("issue_t"):
        own_rows = pl.ds(pl.multiple_of(own * 16, 16), 16)
        for a, b in everyone:
            k, t = device(a, b)
            send(xt_ref.at[t // 2, :, lanes_of(t)], xall.at[own_rows], st, rt, (k, t))
        xall[own_rows, :] = xt_ref[tp // 2, :, lanes_of(tp)]
        tokens = total(xall.at[0:2032], st, rt)

    stage_w = []
    for d in range(1, 4):
        stage_w.append(send(wv_ref, wvz.at[core, chip, 0], sv.at[d], rv.at[d], (kv, along_chips(d))))
        stage_w.append(send(wz_ref, wvz.at[core, chip, 1], sv.at[4 + d], rv.at[4 + d], (kv, along_chips(d))))
    wvz[core, chip, 0] = wv_ref[...]
    wvz[core, chip, 1] = wz_ref[...]
    for n in range(16):
        column = row_to_column(gain_ref[n : n + 1, :].astype(F32))
        gaincol[n * 128 : n * 128 + 128, :] = jnp.broadcast_to(column, (128, 128))
    for c in loads[5:]:
        c.wait()

    saves = []

    def store(g, value):
        rows = slice(g * 512, g * 512 + 512)
        accv[rows, :] = value
        saves.append(pltpu.make_async_copy(accv.at[rows], acc_ref.at[rows], acc_sems.at[g]))
        saves[-1].start()
        abf[g * 512 : g * 512 + 512, :] = value.astype(BF16)

    with jax.named_scope("old"):
        old_part(
            lambda g: state_ref[g * 512 : g * 512 + 512, :],
            lambda g: keys_ref[g * 128 : g * 128 + 128, :],
            [oldv_ref[j].astype(F32) for j in range(4)],
            [logd_ref[j] for j in range(4)],
            [strength_ref[j] for j in range(4)],
            accepted_ref[...],
            store,
        )

    with jax.named_scope("wait_t"):
        tokens.wait_recv()
    with jax.named_scope("project"):
        squares = sum_of([jnp.sum(jnp.square(xall[n * 128 : n * 128 + 128, :].astype(F32)), axis=0, keepdims=True) for n in range(16)])
        scale = lax.rsqrt(squares / 2048.0 + EPS)
        for n in range(16):
            rows = slice(n * 128, n * 128 + 128)
            xnorm[rows, :] = (xall[rows, :].astype(F32) * scale * gaincol[rows, :]).astype(BF16)
        x = xnorm[...]
        qkall[tp, :, 0:128] = dot(x, wq_ref[...], TN).astype(BF16)
        qkall[tp, :, 128:256] = dot(x, wk_ref[...], TN).astype(BF16)
        first = iota((16, 2048), 0) == 0
        wsd = jnp.where(first, jnp.broadcast_to(ws_ref[...].astype(F32), (16, 2048)), jnp.broadcast_to(wd_ref[...].astype(F32), (16, 2048)))
        sdall[tp] = dot(wsd.astype(BF16), x)[0:8]
    stage_c = []
    for d in range(1, 4):
        target = (kv, along_chips(d))
        stage_c.append((send(qkall.at[tp], qkall.at[tp], sq.at[d], rq.at[d], target), send(sdall.at[tp], sdall.at[tp], ssd.at[d], rsd.at[d], target)))
    stage_m = [send(qkall.at[tp], qkall.at[tp], sqm.at[0], rqm.at[0], (kv, mate)), send(sdall.at[tp], sdall.at[tp], sdm.at[0], rdm.at[0], (kv, mate))]
    with jax.named_scope("wait_w"):
        for c in stage_w:
            c.wait_recv()
    to_mate = send(wvz.at[core], wvz.at[core], swm, rwm, (kv, mate))
    with jax.named_scope("wait_wm"):
        to_mate.wait_recv()
    vzs[...] = dot(wvz[...].reshape(256, 2048), xnorm[...]).astype(BF16).reshape(8, 2, 16, 128)
    stage_v = []
    for b in range(1, tp_n):
        _, t = device(0, b)
        stage_v.append(send(vzs.at[lax.rem(t, 2) * 4 + t // 2], vzall.at[tp], svz.at[b], rvz.at[b], (kv, t)))
    vzall[tp] = vzs[core * 4 + chip]
    with jax.named_scope("wait_c"):
        for d in range(1, 4):
            for c in stage_c[d - 1]:
                c.wait_recv()
            source = lax.rem(chip + 4 - d, 4) * 2 + core
            stage_m.append(send(qkall.at[source], qkall.at[source], sqm.at[d], rqm.at[d], (kv, mate)))
            stage_m.append(send(sdall.at[source], sdall.at[source], sdm.at[d], rdm.at[d], (kv, mate)))
    for a in range(kv_n):
        k = lax.rem(kv + a, kv_n)
        for d in range(4):
            if a or d:
                cols = pl.ds(pl.multiple_of(k * 128, 128), 128)
                send(wo_ref.at[:, cols], woall.at[core, kv, chip], so, ro, (k, along_chips(d)))
    woall[core, kv, chip] = wo_ref[:, pl.ds(pl.multiple_of(kv * 128, 128), 128)]
    with jax.named_scope("wait_m"):
        for c in stage_m + stage_v:
            c.wait_recv()

    def query_key(g):
        h, m = divmod(g, 4)
        pieces = [qkall[p * 2 + h, m * 32 : m * 32 + 32, s * 128 : s * 128 + 128] for s in range(2) for p in range(4)]
        return jnp.concatenate(pieces, axis=0)

    def both(f):
        return [jnp.concatenate([f(p * 2), f(p * 2 + 1)], axis=1) for p in range(4)]

    with jax.named_scope("new"):
        outputs = new_part(
            lambda g: abf[g * 512 : g * 512 + 512, :],
            query_key,
            both(lambda t: vzall[t, 0].astype(F32)),
            both(lambda t: sdall[t, 0:1, :]),
            both(lambda t: sdall[t, 1:2, :]),
            rate_ref[...],
            [prop_ref[j] for j in range(4)],
            [parent_ref[j : j + 1, :] for j in range(4)],
        )
        zgate = both(lambda t: vzall[t, 1].astype(F32))
        hgain = jnp.broadcast_to(row_to_column(hgain_ref[...].astype(F32)), (16, 256))
        for t in range(8):
            half = slice((t % 2) * 128, (t % 2) * 128 + 128)
            o, z = outputs[t // 2][:, half], zgate[t // 2][:, half]
            sqs[t] = jnp.sum(jnp.square(o), axis=0, keepdims=True)
            ybuf[t] = (o * hgain[:, half] * (z * jax.nn.sigmoid(z))).astype(BF16)
    with jax.named_scope("issue_e"):
        for a, b in everyone:
            k, t = device(a, b)
            send(sqs.at[t], sqall.at[own], ses, res, (k, t))
            send(ybuf.at[t], yall.at[core, kv, chip], se, re, (k, t))
        sqall[own] = sqs[tp]
        yall[core, kv, chip] = ybuf[tp]
    with jax.named_scope("wait_o"):
        out_weights = total(xall.at[0:1008], so, ro)
        out_weights.wait_recv()
    out_mate = send(woall.at[core], woall.at[core], som, rom, (kv, mate))
    with jax.named_scope("wait_om"):
        out_mate.wait_recv()
    with jax.named_scope("wait_e"):
        all_y, all_sq = total(xall.at[0:2032], se, re), total(sqall.at[0:127], ses, res)
        all_sq.wait_recv()
        all_y.wait_recv()
    with jax.named_scope("combine"):
        for k in range(16):
            scale = lax.rsqrt(sum_of([sqall[k * 8 + t] for t in range(8)]) / 128.0 + EPS)
            for c in range(2):
                for n in range(4):
                    rows = slice(((c * 16 + k) * 4 + n) * 16, ((c * 16 + k) * 4 + n) * 16 + 16)
                    xnorm[rows, :] = (yall[c, k, n].astype(F32) * scale).astype(BF16)
        combined = dot(woall[...].reshape(2048, 128), xnorm[...], TN)
        csend[...] = combined.reshape(8, 16, 128)
        sqf[tp * 16 + kv] = jnp.sum(jnp.square(combined), axis=0, keepdims=True)
    slot = sqf.at[tp * 16 + kv]
    for a, b in everyone:
        send(slot, slot, sh, rh, device(a, b))
    stage_f = []
    for b in range(1, tp_n):
        _, t = device(0, b)
        stage_f.append(send(csend.at[t], call.at[tp], sf.at[b], rf.at[b], (kv, t)))
    call[tp] = csend[tp]
    ogain = jnp.broadcast_to(row_to_column(ogain_ref[...].astype(F32)), (16, 128))
    sums = total(sqf.at[0:127], sh, rh)
    with jax.named_scope("sends"):
        for pair in stage_c:
            for c in pair:
                c.wait_send()
        for c in stage_w + stage_m + stage_v + [tokens, to_mate, out_weights, out_mate, all_y, all_sq]:
            c.wait_send()
    with jax.named_scope("wait_f"):
        for c in stage_f:
            c.wait_recv()
    with jax.named_scope("wait_h"):
        sums.wait_recv()
    for t in range(8):
        scale = lax.rsqrt(sum_of([sqf[t * 16 + k] for k in range(16)]) / 2048.0 + EPS)
        out_ref[t // 2, :, (t % 2) * 128 : (t % 2) * 128 + 128] = (call[t] * scale * ogain).astype(BF16)
    for c in stage_f + [sums]:
        c.wait_send()
    for c in saves:
        c.wait()


def hand_over(out_in, acc_in, out_ref, acc_ref, outv, accv, loaded, saved):
    pieces = [(out_in, outv, out_ref)]
    for g in range(8):
        rows = pl.ds(g * 512, 512)
        pieces.append((acc_in.at[rows], accv.at[rows], acc_ref.at[rows]))
    loads = [pltpu.make_async_copy(a, b, loaded.at[n]) for n, (a, b, _) in enumerate(pieces)]
    saves = [pltpu.make_async_copy(b, c, saved.at[n]) for n, (_, b, c) in enumerate(pieces)]
    for c in loads:
        c.start()
    for load, save in zip(loads, saves):
        load.wait()
        save.start()
    for c in saves:
        c.wait()


def on_device(
    tokens, input_norm_gain, query_weight, key_weight, value_weight, output_gate_weight, strength_weight, decay_weight,
    head_decay_rate, proposal_log_decay, head_norm_gain, output_weight, output_norm_gain, state, previous_keys,
    previous_values, previous_log_decay, previous_strengths, accepted, parent,
):
    tp_n, kv_n = lax.axis_size("tp"), lax.axis_size("kv")
    args = [
        tokens.transpose(1, 2, 0),
        value_weight.transpose(1, 2, 0).reshape(16, 2048),
        output_gate_weight.transpose(1, 2, 0).reshape(16, 2048),
        output_weight.reshape(16, 2048),
        input_norm_gain.reshape(16, 128),
        previous_keys.reshape(1024, 128),
        state.reshape(4096, 128),
        previous_values.transpose(1, 2, 3, 0).reshape(4, 16, 256),
        previous_log_decay.transpose(1, 2, 0),
        previous_strengths.transpose(1, 2, 0),
        accepted.reshape(1, 256),
        query_weight,
        key_weight,
        strength_weight.transpose(1, 0),
        decay_weight.transpose(1, 0),
        head_decay_rate.reshape(1, 1),
        proposal_log_decay.transpose(1, 2, 0),
        parent.transpose(1, 0),
        head_norm_gain.reshape(1, 16),
        output_norm_gain.reshape(1, 16),
    ]
    vmem = pl.BlockSpec(memory_space=pltpu.VMEM)
    hbm = pl.BlockSpec(memory_space=pltpu.HBM)
    specs = [hbm] * len(args)

    def sems(n):
        return [pltpu.SemaphoreType.DMA((n,)), pltpu.SemaphoreType.DMA((n,))]

    def one():
        return [pltpu.SemaphoreType.DMA(()), pltpu.SemaphoreType.DMA(())]

    out, acc = pl.pallas_call(
        functools.partial(kernel, tp_n, kv_n),
        out_shape=(jax.ShapeDtypeStruct((4, 16, 256), BF16), jax.ShapeDtypeStruct((4096, 128), F32)),
        in_specs=specs,
        out_specs=(vmem, hbm),
        scratch_shapes=[
            *[pltpu.VMEM(a.shape, a.dtype) for a in args],
            pltpu.SemaphoreType.DMA((len(args),)),
            pltpu.VMEM((4096, 128), F32),
            pltpu.SemaphoreType.DMA((8,)),
            pltpu.VMEM((2048, 128), BF16),
            pltpu.VMEM((2, 4, 2, 16, 2048), BF16),
            pltpu.VMEM((2, 16, 4, 16, 128), BF16),
            pltpu.VMEM((2048, 128), F32),
            pltpu.VMEM((2048, 128), BF16),
            pltpu.VMEM((8, 128, 256), BF16),
            pltpu.VMEM((8, 2, 16, 128), BF16),
            pltpu.VMEM((8, 2, 16, 128), BF16),
            pltpu.VMEM((8, 8, 128), F32),
            pltpu.VMEM((4096, 128), BF16),
            pltpu.VMEM((8, 16, 128), BF16),
            pltpu.VMEM((2, 16, 4, 16, 128), BF16),
            pltpu.VMEM((8, 1, 128), F32),
            pltpu.VMEM((128, 1, 128), F32),
            pltpu.VMEM((8, 16, 128), F32),
            pltpu.VMEM((8, 16, 128), F32),
            pltpu.VMEM((128, 1, 128), F32),
            *one(), *sems(8), *one(), *sems(4), *sems(4), *sems(4), *sems(4), *sems(8), *one(), *one(), *one(), *one(), *sems(8), *one(),
        ],
        compiler_params=pltpu.CompilerParams(collective_id=0, has_side_effects=True, vmem_limit_bytes=67043328),
    )(*args)
    out, acc = pl.pallas_call(
        hand_over,
        out_shape=(jax.ShapeDtypeStruct((4, 16, 256), BF16), jax.ShapeDtypeStruct((4096, 128), F32)),
        in_specs=(hbm, hbm),
        out_specs=(hbm, hbm),
        scratch_shapes=[pltpu.VMEM((4, 16, 256), BF16), pltpu.VMEM((4096, 128), F32), *sems(9)],
        compiler_params=pltpu.CompilerParams(vmem_limit_bytes=67043328),
    )(out, acc)
    return out.transpose(2, 0, 1), acc.reshape(256, 1, 16, 128)


def solution(mesh):
    placed = (
        P(None, None, ("kv", "tp")),
        P(),
        P(None, "kv"),
        P(None, "kv"),
        P(None, "kv", "tp"),
        P(None, "kv", "tp"),
        P(None, "kv"),
        P(None, "kv"),
        P("kv"),
        P(None, None, "kv"),
        P("tp"),
        P("kv", "tp", None),
        P(("kv", "tp")),
        P(None, "kv", "tp", None),
        P(None, None, "kv"),
        P(None, None, "kv", "tp"),
        P(None, None, "kv"),
        P(None, None, "kv"),
        P(),
        P(),
    )
    return jax.shard_map(
        on_device,
        mesh=mesh,
        in_specs=placed,
        out_specs=(P(None, None, ("kv", "tp")), P(None, "kv", "tp", None)),
        check_vma=False,
    )
```

```python
import functools
import itertools

import jax
import jax.numpy as jnp
from jax import lax
from jax.experimental import pallas as pl
from jax.experimental.pallas import tpu as pltpu
from jax.sharding import PartitionSpec as P

EPS = 1e-06
INPUTS = 19
F32 = jnp.float32
BF16 = jnp.bfloat16
MESH = pl.DeviceIdType.MESH
NT = (((1,), (1,)), ((), ()))
NN = (((1,), (0,)), ((), ()))
TN = (((0,), (0,)), ((), ()))


def dot(a, b, dims=NN):
    return lax.dot_general(a, b, dims, preferred_element_type=F32)


def iota(shape, dim):
    return lax.broadcasted_iota(jnp.int32, shape, dim)


def roll(x, shift):
    return x if shift % 128 == 0 else pltpu.roll(x, shift % 128, 1)


def row_to_column(row):
    n = row.shape[1]
    square = jnp.broadcast_to(row, (n, n))
    return jnp.sum(jnp.where(iota((n, n), 0) == iota((n, n), 1), square, 0.0), axis=1, keepdims=True)


def ungroup(parts, j):
    chunk = iota(parts[0].shape, 1) // 32
    halves = []
    for h in range(2):
        total = None
        for m in range(4):
            x = roll(parts[h * 4 + m], (m - j) * 32)
            total = x if total is None else jnp.where(chunk == m, x, total)
        halves.append(total)
    return jnp.concatenate(halves, axis=1)


def regroup(rows, g):
    h, m = divmod(g, 4)
    total = None
    for j in range(4):
        x = roll(rows[j][:, h * 128 : h * 128 + 128], (j - m) * 32)
        total = x if total is None else jnp.where(iota(x.shape, 1) // 32 == j, x, total)
    return total


def pick_rows(product):
    lanes = product.shape[1]
    cube = product.reshape(32, 16, lanes)
    keep = iota(cube.shape, 0) == iota(cube.shape, 2) % 32
    return jnp.sum(jnp.where(keep, cube, 0.0), axis=0)


def pick_pairs(product):
    n, lanes = product.shape[0] // 32, product.shape[1]
    cube = product.reshape(n, 32, lanes)
    keep = iota(cube.shape, 1) == iota(cube.shape, 2) % 32
    return jnp.sum(jnp.where(keep, cube, 0.0), axis=1)


def sum_of(terms):
    return functools.reduce(lambda a, b: a + b, terms)


def far_first(offsets):
    return sorted([o for o in offsets if any(o)], key=lambda o: -sum(min(d, 4 - d) for d in o[:3]))


def old_part(state, keys, old_values, log_decay, strengths, accepted, store):
    source, target = iota((128, 128), 1), iota((128, 128), 0)
    order = (source == (target % 32) * 4 + target // 32).astype(BF16)
    grouped, reads, grams = [], [], []
    for g in range(8):
        kg = dot(order, keys(g)).astype(BF16)
        grouped.append(kg)
        reads.append(pick_rows(dot(state(g).astype(BF16), kg, NT)))
        grams.append(pick_pairs(dot(kg, kg, NT)))
    gram = [ungroup(grams, j) for j in range(4)]
    read = [ungroup(reads, j) for j in range(4)]
    inv = [lax.rsqrt(gram[j][j : j + 1] + EPS) for j in range(4)]
    gam, beta = [], []
    for j in range(4):
        live = (j < accepted).astype(F32)
        g_j = log_decay[j] * live
        gam.append(g_j if j == 0 else gam[-1] + g_j)
        beta.append(strengths[j] * live)
    update = []
    for i in range(4):
        u = beta[i] * (old_values[i] - (jnp.exp(gam[i]) * inv[i]) * read[i])
        for j in range(i):
            a = beta[i] * (gram[j][i : i + 1] * (inv[i] * inv[j])) * jnp.exp(gam[i] - gam[j])
            u = u - a * update[j]
        update.append(u)
    weighted = [update[j] * (jnp.exp(gam[3] - gam[j]) * inv[j]) for j in range(4)]
    kept = jnp.exp(gam[3])
    columns = [jnp.broadcast_to(row_to_column(kept[:, h * 128 : h * 128 + 128]), (128, 128)) for h in range(2)]
    for g in range(8):
        wg = regroup(weighted, g)
        cube = (32, 16, 128)
        keep = iota(cube, 0) == iota(cube, 2) % 32
        block = jnp.where(keep, jnp.broadcast_to(wg[None], cube), 0.0).reshape(512, 128).astype(BF16)
        h, m = divmod(g, 4)
        scale = jnp.broadcast_to(columns[h][m * 32 : m * 32 + 32][:, None, :], cube).reshape(512, 128)
        store(g, scale * state(g) + dot(block, grouped[g]))


def new_part(accepted_state, query_key, values, beta_pre, decay_pre, rate, proposal, parent):
    reads, grams = [], []
    for g in range(8):
        qk = query_key(g)
        reads.append(pick_rows(dot(accepted_state(g), qk, NT)))
        grams.append(pick_pairs(dot(qk, qk, NT)))
    left = [r[:, :128] for r in reads], [r[:, 128:] for r in reads]
    aq = [ungroup(left[0], j) for j in range(4)]
    ak = [ungroup(left[1], j) for j in range(4)]
    gq = [ungroup([r[:, :128] for r in grams], j) for j in range(4)]
    gk = [ungroup([r[:, 128:] for r in grams], j) for j in range(4)]
    inv_q = [lax.rsqrt(gq[j][j : j + 1] + EPS) * (128.0**-0.5) for j in range(4)]
    inv_k = [lax.rsqrt(gk[j][4 + j : 5 + j] + EPS) for j in range(4)]
    ancestors = []
    for i in range(4):
        row = {j: (parent[i] == j).astype(F32) for j in range(i)}
        row = {j: row[j] + sum_of([jnp.zeros_like(row[j])] + [row[m] * ancestors[m][j] for m in range(j + 1, i)]) for j in range(i)}
        ancestors.append(row)
    beta, g_new, gam = [], [], []
    for i in range(4):
        x = decay_pre[i]
        softplus = jnp.maximum(x, 0.0) + jnp.log1p(jnp.exp(-jnp.abs(x)))
        g_new.append(-rate * softplus + proposal[i])
        beta.append(jax.nn.sigmoid(beta_pre[i]))
        gam.append(sum_of([g_new[i]] + [ancestors[i][j] * g_new[j] for j in range(i)]))
    outputs, update = [], []
    for i in range(4):
        grow = jnp.exp(gam[i])
        u = beta[i] * (values[i] - (grow * inv_k[i]) * ak[i])
        o = (grow * inv_q[i]) * aq[i]
        for j in range(i):
            reach = jnp.exp(jnp.minimum(gam[i] - gam[j], 0.0)) * ancestors[i][j] * inv_k[j]
            u = u - (beta[i] * inv_k[i] * gk[j][4 + i : 5 + i] * reach) * update[j]
            o = o + (inv_q[i] * gk[j][i : i + 1] * reach) * update[j]
        update.append(u)
        o = o + (inv_q[i] * gk[i][i : i + 1] * inv_k[i]) * u
        outputs.append(o)
    return outputs


def kernel(
    tp_n, kv_n, *refs,
):
    run(tp_n, kv_n, refs[:INPUTS], *refs[INPUTS:])


def run(
    tp_n, kv_n, sources, sums_ref, comb_ref, acc_ref,
    xt_ref, wv_ref, wz_ref, wo_ref, gain_ref, keys_ref, state_ref, oldv_ref, logd_ref, strength_ref, accepted_ref,
    wq_ref, wk_ref, ws_ref, wd_ref, rate_ref, prop_ref, parent_ref, hgain_ref,
    load_sems, accv, acc_sems,
    xall, wvz, woall, gaincol, xnorm, qkall, vzs, vzall, sdall, abf, ybuf, yall, sqs, sqall, csend, sqf,
    st, rt, sv, rv, swm, rwm, sq, rq, ssd, rsd, sqm, rqm, sdm, rdm, svz, rvz, so, ro, som, rom, se, re, ses, res, sf, rf, sh, rh,
):
    held = (
        xt_ref, wv_ref, wz_ref, wo_ref, gain_ref, keys_ref, state_ref, oldv_ref, logd_ref, strength_ref, accepted_ref,
        wq_ref, wk_ref, ws_ref, wd_ref, rate_ref, prop_ref, parent_ref, hgain_ref,
    )
    loads = [pltpu.make_async_copy(src, dst, load_sems.at[n]) for n, (src, dst) in enumerate(zip(sources, held))]
    kv, tp = lax.axis_index("kv"), lax.axis_index("tp")
    chip, core = tp // 2, lax.rem(tp, 2)
    mate = tp + 1 - 2 * core
    own = kv * tp_n + tp
    everyone = far_first(itertools.product(range(4), range(4), range(4), range(2)))
    high, low = kv // 4, lax.rem(kv, 4)

    def device(offset):
        z, y, x, c = offset
        return lax.rem(high + z, 4) * 4 + lax.rem(low + y, 4), lax.rem(chip + x, 4) * 2 + lax.rem(core + c, 2)

    def send(src, dst, send_sem, recv_sem, target):
        c = remote(src, dst, send_sem, recv_sem, target)
        c.start()
        return c

    def remote(src, dst, send_sem, recv_sem, target):
        return pltpu.make_async_remote_copy(
            src_ref=src, dst_ref=dst, send_sem=send_sem, recv_sem=recv_sem, device_id=target, device_id_type=MESH
        )

    def total(ref, send_sem, recv_sem):
        return remote(ref, ref, send_sem, recv_sem, (kv, mate))

    def along_chips(d):
        return lax.rem(chip + d, 4) * 2 + core

    def lanes_of(t):
        return pl.ds(pl.multiple_of(lax.rem(t, 2) * 128, 128), 128)

    barrier = pltpu.get_barrier_semaphore()
    for c in loads[:5]:
        c.start()
    for o in everyone:
        pl.semaphore_signal(barrier, inc=1, device_id=device(o), device_id_type=MESH)
    for c in loads[5:]:
        c.start()
    for c in loads[:5]:
        c.wait()
    with jax.named_scope("barrier"):
        pl.semaphore_wait(barrier, kv_n * tp_n - 1)

    with jax.named_scope("issue_t"):
        own_rows = pl.ds(pl.multiple_of(own * 16, 16), 16)
        for o in everyone:
            k, t = device(o)
            send(xt_ref.at[t // 2, :, lanes_of(t)], xall.at[own_rows], st, rt, (k, t))
        xall[own_rows, :] = xt_ref[tp // 2, :, lanes_of(tp)]
        tokens = total(xall.at[0:2032], st, rt)

    for o in far_first(itertools.product(range(4), range(4), [0], [0])):
        k, _ = device(o)
        cols = pl.ds(pl.multiple_of(k * 128, 128), 128)
        send(wo_ref.at[:, cols], woall.at[core, chip, kv], so, ro, (k, tp))
    woall[core, chip, kv] = wo_ref[:, pl.ds(pl.multiple_of(kv * 128, 128), 128)]

    stage_w, stage_wm = [], []
    for d in (2, 1, 3):
        target = (kv, along_chips(d))
        stage_w.append(
            [
                send(wv_ref, wvz.at[core, chip, 0], sv.at[d], rv.at[d], target),
                send(wz_ref, wvz.at[core, chip, 1], sv.at[4 + d], rv.at[4 + d], target),
            ]
        )
    stage_wm.append(send(wv_ref, wvz.at[core, chip, 0], swm.at[0], rwm.at[0], (kv, mate)))
    stage_wm.append(send(wz_ref, wvz.at[core, chip, 1], swm.at[4], rwm.at[4], (kv, mate)))
    wvz[core, chip, 0] = wv_ref[...]
    wvz[core, chip, 1] = wz_ref[...]
    for n in range(16):
        column = row_to_column(gain_ref[n : n + 1, :].astype(F32))
        gaincol[n * 128 : n * 128 + 128, :] = jnp.broadcast_to(column, (128, 128))
    for c in loads[5:]:
        c.wait()

    saves = []

    def store(g, value):
        rows = slice(g * 512, g * 512 + 512)
        accv[rows, :] = value
        saves.append(pltpu.make_async_copy(accv.at[rows], acc_ref.at[rows], acc_sems.at[g]))
        saves[-1].start()
        abf[g * 512 : g * 512 + 512, :] = value.astype(BF16)

    with jax.named_scope("old"):
        old_part(
            lambda g: state_ref[g * 512 : g * 512 + 512, :],
            lambda g: keys_ref[g * 128 : g * 128 + 128, :],
            [oldv_ref[j].astype(F32) for j in range(4)],
            [logd_ref[j] for j in range(4)],
            [strength_ref[j] for j in range(4)],
            accepted_ref[...],
            store,
        )

    with jax.named_scope("wait_t"):
        tokens.wait_recv()
    with jax.named_scope("project"):
        squares = sum_of([jnp.sum(jnp.square(xall[n * 128 : n * 128 + 128, :].astype(F32)), axis=0, keepdims=True) for n in range(16)])
        scale = lax.rsqrt(squares / 2048.0 + EPS)
        for n in range(16):
            rows = slice(n * 128, n * 128 + 128)
            xnorm[rows, :] = (xall[rows, :].astype(F32) * scale * gaincol[rows, :]).astype(BF16)
        x = xnorm[...]
        qkall[tp, :, 0:128] = dot(x, wq_ref[...], TN).astype(BF16)
        qkall[tp, :, 128:256] = dot(x, wk_ref[...], TN).astype(BF16)
        first = iota((16, 2048), 0) == 0
        wsd = jnp.where(first, jnp.broadcast_to(ws_ref[...].astype(F32), (16, 2048)), jnp.broadcast_to(wd_ref[...].astype(F32), (16, 2048)))
        sdall[tp] = dot(wsd.astype(BF16), x)[0:8]
    stage_c = []
    for d in (2, 1, 3):
        target = (kv, along_chips(d))
        stage_c.append((send(qkall.at[tp], qkall.at[tp], sq.at[d], rq.at[d], target), send(sdall.at[tp], sdall.at[tp], ssd.at[d], rsd.at[d], target)))
    stage_m = [send(qkall.at[tp], qkall.at[tp], sqm.at[0], rqm.at[0], (kv, mate)), send(sdall.at[tp], sdall.at[tp], sdm.at[0], rdm.at[0], (kv, mate))]
    with jax.named_scope("wait_w"):
        for d, pair in ((1, stage_w[1]), (3, stage_w[2]), (2, stage_w[0])):
            for c in pair:
                c.wait_recv()
            block = wvz.at[core, lax.rem(chip + 4 - d, 4)]
            stage_wm.append(send(block, block, swm.at[d], rwm.at[d], (kv, mate)))
    with jax.named_scope("wait_wm"):
        for c in stage_wm:
            c.wait_recv()
    vzs[...] = dot(wvz[...].reshape(256, 2048), xnorm[...]).astype(BF16).reshape(8, 2, 16, 128)
    stage_v = []
    along_tp = far_first(itertools.product([0], [0], range(4), range(2)))
    for b, o in enumerate(along_tp):
        _, t = device(o)
        stage_v.append(send(vzs.at[lax.rem(t, 2) * 4 + t // 2], vzall.at[tp], svz.at[b], rvz.at[b], (kv, t)))
    vzall[tp] = vzs[core * 4 + chip]
    with jax.named_scope("wait_c"):
        for d, pair in ((1, stage_c[1]), (3, stage_c[2]), (2, stage_c[0])):
            for c in pair:
                c.wait_recv()
            source = lax.rem(chip + 4 - d, 4) * 2 + core
            stage_m.append(send(qkall.at[source], qkall.at[source], sqm.at[d], rqm.at[d], (kv, mate)))
            stage_m.append(send(sdall.at[source], sdall.at[source], sdm.at[d], rdm.at[d], (kv, mate)))
    out_tiles = total(xall.at[0:240], so, ro)
    out_tiles.wait_recv()
    block = woall.at[core, chip]
    stage_o = [send(block, block, som.at[d], rom.at[d], (kv, along_chips(d))) for d in (2, 1, 3)]
    stage_o.append(send(block, block, som.at[0], rom.at[0], (kv, mate)))
    with jax.named_scope("wait_m"):
        for c in stage_m + stage_v:
            c.wait_recv()

    def query_key(g):
        h, m = divmod(g, 4)
        pieces = [qkall[p * 2 + h, m * 32 : m * 32 + 32, s * 128 : s * 128 + 128] for s in range(2) for p in range(4)]
        return jnp.concatenate(pieces, axis=0)

    def both(f):
        return [jnp.concatenate([f(p * 2), f(p * 2 + 1)], axis=1) for p in range(4)]

    with jax.named_scope("new"):
        outputs = new_part(
            lambda g: abf[g * 512 : g * 512 + 512, :],
            query_key,
            both(lambda t: vzall[t, 0].astype(F32)),
            both(lambda t: sdall[t, 0:1, :]),
            both(lambda t: sdall[t, 1:2, :]),
            rate_ref[...],
            [prop_ref[j] for j in range(4)],
            [parent_ref[j : j + 1, :] for j in range(4)],
        )
        zgate = both(lambda t: vzall[t, 1].astype(F32))
        hgain = jnp.broadcast_to(row_to_column(hgain_ref[...].astype(F32)), (16, 256))
        for t in range(8):
            half = slice((t % 2) * 128, (t % 2) * 128 + 128)
            o, z = outputs[t // 2][:, half], zgate[t // 2][:, half]
            sqs[t] = jnp.sum(jnp.square(o), axis=0, keepdims=True)
            ybuf[t] = (o * hgain[:, half] * (z * jax.nn.sigmoid(z))).astype(BF16)
    with jax.named_scope("issue_e"):
        for o in everyone:
            k, t = device(o)
            send(sqs.at[t], sqall.at[own], ses, res, (k, t))
            send(ybuf.at[t], yall.at[core, chip, kv], se, re, (k, t))
        sqall[own] = sqs[tp]
        yall[core, chip, kv] = ybuf[tp]
    with jax.named_scope("wait_o"):
        for d, c in ((1, stage_o[1]), (3, stage_o[2]), (2, stage_o[0])):
            c.wait_recv()
            block = woall.at[core, lax.rem(chip + 4 - d, 4)]
            stage_o.append(send(block, block, som.at[3 + d], rom.at[3 + d], (kv, mate)))
        for c in stage_o[3:]:
            c.wait_recv()
    with jax.named_scope("wait_e"):
        all_y, all_sq = total(xall.at[0:2032], se, re), total(sqall.at[0:127], ses, res)
        all_sq.wait_recv()
        all_y.wait_recv()
    with jax.named_scope("combine"):
        for k in range(16):
            scale = lax.rsqrt(sum_of([sqall[k * 8 + t] for t in range(8)]) / 128.0 + EPS)
            for c in range(2):
                for n in range(4):
                    rows = slice(((c * 4 + n) * 16 + k) * 16, ((c * 4 + n) * 16 + k) * 16 + 16)
                    xnorm[rows, :] = (yall[c, n, k].astype(F32) * scale).astype(BF16)
        combined = dot(woall[...].reshape(2048, 128), xnorm[...], TN)
        csend[...] = combined.reshape(8, 16, 128)
        sqf[...] = jnp.sum(jnp.square(combined), axis=0, keepdims=True)
    for o in everyone:
        send(sqf, sums_ref.at[tp * 16 + kv], sh, rh, device(o))
    stage_f = []
    for b, o in enumerate(along_tp):
        _, t = device(o)
        stage_f.append(send(csend.at[t], comb_ref.at[tp], sf.at[b], rf.at[b], (kv, t)))
    saves.append(pltpu.make_async_copy(sqf, sums_ref.at[tp * 16 + kv], load_sems.at[0]))
    saves.append(pltpu.make_async_copy(csend.at[tp], comb_ref.at[tp], load_sems.at[1]))
    for c in saves[-2:]:
        c.start()
    sums = total(sqall.at[0:127], sh, rh)
    with jax.named_scope("sends"):
        for pair in stage_c + stage_w:
            for c in pair:
                c.wait_send()
        for c in stage_wm + stage_m + stage_v + stage_o + [tokens, out_tiles, all_y, all_sq]:
            c.wait_send()
        for c in saves:
            c.wait()
    with jax.named_scope("wait_f"):
        for c in stage_f:
            c.wait_recv()
    with jax.named_scope("wait_h"):
        sums.wait_recv()
    for c in stage_f + [sums]:
        c.wait_send()


def finish(sums_in, comb_in, gain_in, acc_in, out_ref, acc_ref, sums, comb, gain, outv, accv, loaded, saved):
    pieces = [(sums_in, sums), (comb_in, comb), (gain_in, gain)]
    blocks = [pl.ds(g * 512, 512) for g in range(8)]
    pieces += [(acc_in.at[rows], accv.at[rows]) for rows in blocks]
    loads = [pltpu.make_async_copy(a, b, loaded.at[n]) for n, (a, b) in enumerate(pieces)]
    saves = [pltpu.make_async_copy(accv.at[rows], acc_ref.at[rows], saved.at[g]) for g, rows in enumerate(blocks)]
    saves.append(pltpu.make_async_copy(outv, out_ref, saved.at[8]))
    for c in loads:
        c.start()
    for c in loads[:3]:
        c.wait()
    column = jnp.broadcast_to(row_to_column(gain[...].astype(F32)), (16, 128))
    for t in range(8):
        scale = lax.rsqrt(sum_of([sums[t * 16 + k] for k in range(16)]) / 2048.0 + EPS)
        outv[t // 2, :, (t % 2) * 128 : (t % 2) * 128 + 128] = (comb[t] * scale * column).astype(BF16)
    saves[8].start()
    for load, save in zip(loads[3:], saves):
        load.wait()
        save.start()
    for c in saves:
        c.wait()


def on_device(
    tokens, input_norm_gain, query_weight, key_weight, value_weight, output_gate_weight, strength_weight, decay_weight,
    head_decay_rate, proposal_log_decay, head_norm_gain, output_weight, output_norm_gain, state, previous_keys,
    previous_values, previous_log_decay, previous_strengths, accepted, parent,
):
    tp_n, kv_n = lax.axis_size("tp"), lax.axis_size("kv")
    args = [
        tokens.transpose(1, 2, 0),
        value_weight.transpose(1, 2, 0).reshape(16, 2048),
        output_gate_weight.transpose(1, 2, 0).reshape(16, 2048),
        output_weight.reshape(16, 2048),
        input_norm_gain.reshape(16, 128),
        previous_keys.reshape(1024, 128),
        state.reshape(4096, 128),
        previous_values.transpose(1, 2, 3, 0).reshape(4, 16, 256),
        previous_log_decay.transpose(1, 2, 0),
        previous_strengths.transpose(1, 2, 0),
        accepted.reshape(1, 256),
        query_weight,
        key_weight,
        strength_weight.transpose(1, 0),
        decay_weight.transpose(1, 0),
        head_decay_rate.reshape(1, 1),
        proposal_log_decay.transpose(1, 2, 0),
        parent.transpose(1, 0),
        head_norm_gain.reshape(1, 16),
    ]
    hbm = pl.BlockSpec(memory_space=pltpu.HBM)
    specs = [hbm] * len(args)

    def sems(n):
        return [pltpu.SemaphoreType.DMA((n,)), pltpu.SemaphoreType.DMA((n,))]

    def one():
        return [pltpu.SemaphoreType.DMA(()), pltpu.SemaphoreType.DMA(())]

    sums, combined, acc = pl.pallas_call(
        functools.partial(kernel, tp_n, kv_n),
        out_shape=(
            jax.ShapeDtypeStruct((128, 1, 128), F32),
            jax.ShapeDtypeStruct((8, 16, 128), F32),
            jax.ShapeDtypeStruct((4096, 128), F32),
        ),
        in_specs=specs,
        out_specs=(hbm, hbm, hbm),
        scratch_shapes=[
            *[pltpu.VMEM(a.shape, a.dtype) for a in args],
            pltpu.SemaphoreType.DMA((len(args),)),
            pltpu.VMEM((4096, 128), F32),
            pltpu.SemaphoreType.DMA((8,)),
            pltpu.VMEM((2048, 128), BF16),
            pltpu.VMEM((2, 4, 2, 16, 2048), BF16),
            pltpu.VMEM((2, 4, 16, 16, 128), BF16),
            pltpu.VMEM((2048, 128), F32),
            pltpu.VMEM((2048, 128), BF16),
            pltpu.VMEM((8, 128, 256), BF16),
            pltpu.VMEM((8, 2, 16, 128), BF16),
            pltpu.VMEM((8, 2, 16, 128), BF16),
            pltpu.VMEM((8, 8, 128), F32),
            pltpu.VMEM((4096, 128), BF16),
            pltpu.VMEM((8, 16, 128), BF16),
            pltpu.VMEM((2, 4, 16, 16, 128), BF16),
            pltpu.VMEM((8, 1, 128), F32),
            pltpu.VMEM((128, 1, 128), F32),
            pltpu.VMEM((8, 16, 128), F32),
            pltpu.VMEM((1, 128), F32),
            *one(), *sems(8), *sems(5), *sems(4), *sems(4), *sems(4), *sems(4), *sems(8), *one(), *sems(7), *one(), *one(), *sems(8), *one(),
        ],
        compiler_params=pltpu.CompilerParams(collective_id=0, has_side_effects=True, vmem_limit_bytes=67043328),
    )(*args)
    out, acc = pl.pallas_call(
        finish,
        out_shape=(jax.ShapeDtypeStruct((4, 16, 256), BF16), jax.ShapeDtypeStruct((4096, 128), F32)),
        in_specs=(hbm,) * 4,
        out_specs=(hbm, hbm),
        scratch_shapes=[
            pltpu.VMEM((128, 1, 128), F32),
            pltpu.VMEM((8, 16, 128), F32),
            pltpu.VMEM((1, 16), BF16),
            pltpu.VMEM((4, 16, 256), BF16),
            pltpu.VMEM((4096, 128), F32),
            pltpu.SemaphoreType.DMA((11,)),
            pltpu.SemaphoreType.DMA((9,)),
        ],
        compiler_params=pltpu.CompilerParams(vmem_limit_bytes=67043328),
    )(sums, combined, output_norm_gain.reshape(1, 16), acc)
    return out.transpose(2, 0, 1), acc.reshape(256, 1, 16, 128)


def solution(mesh):
    placed = (
        P(None, None, ("kv", "tp")),
        P(),
        P(None, "kv"),
        P(None, "kv"),
        P(None, "kv", "tp"),
        P(None, "kv", "tp"),
        P(None, "kv"),
        P(None, "kv"),
        P("kv"),
        P(None, None, "kv"),
        P("tp"),
        P("kv", "tp", None),
        P(("kv", "tp")),
        P(None, "kv", "tp", None),
        P(None, None, "kv"),
        P(None, None, "kv", "tp"),
        P(None, None, "kv"),
        P(None, None, "kv"),
        P(),
        P(),
    )
    return jax.shard_map(
        on_device,
        mesh=mesh,
        in_specs=placed,
        out_specs=(P(None, None, ("kv", "tp")), P(None, "kv", "tp", None)),
        check_vma=False,
    )
```

```python
import functools
import itertools

import jax
import jax.numpy as jnp
from jax import lax
from jax.experimental import pallas as pl
from jax.experimental.pallas import tpu as pltpu
from jax.sharding import PartitionSpec as P

EPS = 1e-06
INPUTS = 19
F32 = jnp.float32
BF16 = jnp.bfloat16
MESH = pl.DeviceIdType.MESH
NT = (((1,), (1,)), ((), ()))
NN = (((1,), (0,)), ((), ()))
TN = (((0,), (0,)), ((), ()))


def dot(a, b, dims=NN):
    return lax.dot_general(a, b, dims, preferred_element_type=F32)


def iota(shape, dim):
    return lax.broadcasted_iota(jnp.int32, shape, dim)


def roll(x, shift):
    return x if shift % 128 == 0 else pltpu.roll(x, shift % 128, 1)


def row_to_column(row):
    n = row.shape[1]
    square = jnp.broadcast_to(row, (n, n))
    return jnp.sum(jnp.where(iota((n, n), 0) == iota((n, n), 1), square, 0.0), axis=1, keepdims=True)


def ungroup_half(parts, j):
    chunk = iota(parts[0].shape, 1) // 32
    total = parts[0] if j == 0 else roll(parts[0], -j * 32)
    for m in range(1, 4):
        total = jnp.where(chunk == m, roll(parts[m], (m - j) * 32), total)
    return total


def ungroup(parts, j):
    return jnp.concatenate([ungroup_half(parts[:4], j), ungroup_half(parts[4:], j)], axis=1)


def regroup(rows, g):
    h, m = divmod(g, 4)
    total = None
    for j in range(4):
        x = roll(rows[j][:, h * 128 : h * 128 + 128], (j - m) * 32)
        total = x if total is None else jnp.where(iota(x.shape, 1) // 32 == j, x, total)
    return total


def pick_rows(product):
    lanes = product.shape[1]
    cube = product.reshape(32, 16, lanes)
    keep = iota(cube.shape, 0) == iota(cube.shape, 2) % 32
    return jnp.sum(jnp.where(keep, cube, 0.0), axis=0)


def pick_pairs(product):
    n, lanes = product.shape[0] // 32, product.shape[1]
    cube = product.reshape(n, 32, lanes)
    keep = iota(cube.shape, 1) == iota(cube.shape, 2) % 32
    return jnp.sum(jnp.where(keep, cube, 0.0), axis=1)


def sum_of(terms):
    return functools.reduce(lambda a, b: a + b, terms)


def far_first(offsets):
    return sorted([o for o in offsets if any(o)], key=lambda o: -sum(min(d, 4 - d) for d in o[:3]))


def old_part(state, keys, old_values, log_decay, strengths, accepted, store):
    source, target = iota((128, 128), 1), iota((128, 128), 0)
    order = (source == (target % 32) * 4 + target // 32).astype(BF16)
    grouped, reads, grams = [], [], []
    for g in range(8):
        kg = dot(order, keys(g)).astype(BF16)
        grouped.append(kg)
        reads.append(pick_rows(dot(state(g).astype(BF16), kg, NT)))
        grams.append(pick_pairs(dot(kg, kg, NT)))
    gram = [ungroup(grams, j) for j in range(4)]
    read = [ungroup(reads, j) for j in range(4)]
    inv = [lax.rsqrt(gram[j][j : j + 1] + EPS) for j in range(4)]
    gam, beta = [], []
    for j in range(4):
        live = (j < accepted).astype(F32)
        g_j = log_decay[j] * live
        gam.append(g_j if j == 0 else gam[-1] + g_j)
        beta.append(strengths[j] * live)
    update = []
    for i in range(4):
        u = beta[i] * (old_values[i] - (jnp.exp(gam[i]) * inv[i]) * read[i])
        for j in range(i):
            a = beta[i] * (gram[j][i : i + 1] * (inv[i] * inv[j])) * jnp.exp(gam[i] - gam[j])
            u = u - a * update[j]
        update.append(u)
    weighted = [update[j] * (jnp.exp(gam[3] - gam[j]) * inv[j]) for j in range(4)]
    kept = jnp.exp(gam[3])
    columns = [jnp.broadcast_to(row_to_column(kept[:, h * 128 : h * 128 + 128]), (128, 128)) for h in range(2)]
    for g in range(8):
        wg = regroup(weighted, g)
        cube = (32, 16, 128)
        keep = iota(cube, 0) == iota(cube, 2) % 32
        block = jnp.where(keep, jnp.broadcast_to(wg[None], cube), 0.0).reshape(512, 128).astype(BF16)
        h, m = divmod(g, 4)
        scale = jnp.broadcast_to(columns[h][m * 32 : m * 32 + 32][:, None, :], cube).reshape(512, 128)
        store(g, scale * state(g) + dot(block, grouped[g]))


def new_part(accepted_state, query_key, values, beta_pre, decay_pre, rate, proposal, parent):
    reads, grams = [], []
    for m in range(4):
        qk = query_key(m)
        reads.append(pick_rows(dot(accepted_state(m), qk, NT)))
        grams.append(pick_pairs(dot(qk, qk, NT)))
    aq = [ungroup_half([r[:, :128] for r in reads], j) for j in range(4)]
    ak = [ungroup_half([r[:, 128:] for r in reads], j) for j in range(4)]
    gq = [ungroup_half([r[:, :128] for r in grams], j) for j in range(4)]
    gk = [ungroup_half([r[:, 128:] for r in grams], j) for j in range(4)]
    inv_q = [lax.rsqrt(gq[j][j : j + 1] + EPS) * (128.0**-0.5) for j in range(4)]
    inv_k = [lax.rsqrt(gk[j][4 + j : 5 + j] + EPS) for j in range(4)]
    ancestors = []
    for i in range(4):
        row = {j: (parent[i] == j).astype(F32) for j in range(i)}
        row = {j: row[j] + sum_of([jnp.zeros_like(row[j])] + [row[m] * ancestors[m][j] for m in range(j + 1, i)]) for j in range(i)}
        ancestors.append(row)
    beta, g_new, gam = [], [], []
    for i in range(4):
        x = decay_pre[i]
        softplus = jnp.maximum(x, 0.0) + jnp.log1p(jnp.exp(-jnp.abs(x)))
        g_new.append(-rate * softplus + proposal[i])
        beta.append(jax.nn.sigmoid(beta_pre[i]))
        gam.append(sum_of([g_new[i]] + [ancestors[i][j] * g_new[j] for j in range(i)]))
    outputs, update = [], []
    for i in range(4):
        grow = jnp.exp(gam[i])
        u = beta[i] * (values[i] - (grow * inv_k[i]) * ak[i])
        o = (grow * inv_q[i]) * aq[i]
        for j in range(i):
            reach = jnp.exp(jnp.minimum(gam[i] - gam[j], 0.0)) * ancestors[i][j] * inv_k[j]
            u = u - (beta[i] * inv_k[i] * gk[j][4 + i : 5 + i] * reach) * update[j]
            o = o + (inv_q[i] * gk[j][i : i + 1] * reach) * update[j]
        update.append(u)
        o = o + (inv_q[i] * gk[i][i : i + 1] * inv_k[i]) * u
        outputs.append(o)
    return outputs


def kernel(
    tp_n, kv_n, *refs,
):
    run(tp_n, kv_n, refs[:INPUTS], *refs[INPUTS:])


def run(
    tp_n, kv_n, sources, sums_ref, comb_ref, acc_ref,
    xt_ref, wv_ref, wz_ref, wo_ref, gain_ref, keys_ref, state_ref, oldv_ref, logd_ref, strength_ref, accepted_ref,
    wq_ref, wk_ref, ws_ref, wd_ref, rate_ref, prop_ref, parent_ref, hgain_ref,
    load_sems, accv, acc_sems,
    xall, wvz, woall, gaincol, xnorm, xmate, ynorm, qkall, vzs, vzall, sdall, abf, ybuf, yall, sqs, sqall, csend, sqf,
    st, rt, sv, rv, swm, rwm, sq, rq, ssd, rsd, sqm, rqm, sdm, rdm, svz, rvz, so, ro, som, rom, se, re, ses, res, sf, rf, sh, rh,
):
    held = (
        xt_ref, wv_ref, wz_ref, wo_ref, gain_ref, keys_ref, state_ref, oldv_ref, logd_ref, strength_ref, accepted_ref,
        wq_ref, wk_ref, ws_ref, wd_ref, rate_ref, prop_ref, parent_ref, hgain_ref,
    )
    loads = [pltpu.make_async_copy(src, dst, load_sems.at[n]) for n, (src, dst) in enumerate(zip(sources, held))]
    kv, tp = lax.axis_index("kv"), lax.axis_index("tp")
    chip, core = tp // 2, lax.rem(tp, 2)
    mate = tp + 1 - 2 * core
    own = kv * tp_n + tp
    everyone = far_first(itertools.product(range(4), range(4), range(4), range(2)))
    high, low = kv // 4, lax.rem(kv, 4)

    def device(offset):
        z, y, x, c = offset
        return lax.rem(high + z, 4) * 4 + lax.rem(low + y, 4), lax.rem(chip + x, 4) * 2 + lax.rem(core + c, 2)

    def send(src, dst, send_sem, recv_sem, target):
        c = remote(src, dst, send_sem, recv_sem, target)
        c.start()
        return c

    def remote(src, dst, send_sem, recv_sem, target):
        return pltpu.make_async_remote_copy(
            src_ref=src, dst_ref=dst, send_sem=send_sem, recv_sem=recv_sem, device_id=target, device_id_type=MESH
        )

    def total(ref, send_sem, recv_sem):
        return remote(ref, ref, send_sem, recv_sem, (kv, mate))

    def along_chips(d):
        return lax.rem(chip + d, 4) * 2 + core

    def lanes_of(t):
        return pl.ds(pl.multiple_of(lax.rem(t, 2) * 128, 128), 128)

    barrier = pltpu.get_barrier_semaphore()
    for c in loads[:5]:
        c.start()
    for o in everyone:
        pl.semaphore_signal(barrier, inc=1, device_id=device(o), device_id_type=MESH)
    for c in loads[5:]:
        c.start()
    for c in loads[:5]:
        c.wait()
    with jax.named_scope("barrier"):
        pl.semaphore_wait(barrier, kv_n * tp_n - 1)

    with jax.named_scope("issue_t"):
        own_rows = pl.ds(pl.multiple_of(own * 16, 16), 16)
        for o in everyone:
            k, t = device(o)
            send(xt_ref.at[t // 2, :, lanes_of(t)], xall.at[own_rows], st, rt, (k, t))
        xall[own_rows, :] = xt_ref[tp // 2, :, lanes_of(tp)]
        tokens = total(xall.at[0:2032], st, rt)

    for o in far_first(itertools.product(range(4), range(4), [0], [0])):
        k, _ = device(o)
        cols = pl.ds(pl.multiple_of(k * 128, 128), 128)
        send(wo_ref.at[:, cols], woall.at[core, chip, kv], so, ro, (k, tp))
    woall[core, chip, kv] = wo_ref[:, pl.ds(pl.multiple_of(kv * 128, 128), 128)]

    stage_w = []
    for d in (2, 1, 3):
        target = (kv, along_chips(d))
        stage_w.append(send(wv_ref, wvz.at[chip, 0], sv.at[d], rv.at[d], target))
        stage_w.append(send(wz_ref, wvz.at[chip, 1], sv.at[4 + d], rv.at[4 + d], target))
    wvz[chip, 0] = wv_ref[...]
    wvz[chip, 1] = wz_ref[...]
    for n in range(16):
        column = row_to_column(gain_ref[n : n + 1, :].astype(F32))
        gaincol[n * 128 : n * 128 + 128, :] = jnp.broadcast_to(column, (128, 128))
    for c in loads[5:]:
        c.wait()

    saves = []

    def store(g, value):
        rows = slice(g * 512, g * 512 + 512)
        accv[rows, :] = value
        saves.append(pltpu.make_async_copy(accv.at[rows], acc_ref.at[rows], acc_sems.at[g]))
        saves[-1].start()
        abf[g * 512 : g * 512 + 512, :] = value.astype(BF16)

    with jax.named_scope("old"):
        old_part(
            lambda g: state_ref[g * 512 : g * 512 + 512, :],
            lambda g: keys_ref[g * 128 : g * 128 + 128, :],
            [oldv_ref[j].astype(F32) for j in range(4)],
            [logd_ref[j] for j in range(4)],
            [strength_ref[j] for j in range(4)],
            accepted_ref[...],
            store,
        )

    with jax.named_scope("wait_t"):
        tokens.wait_recv()
    with jax.named_scope("project"):
        squares = sum_of([jnp.sum(jnp.square(xall[n * 128 : n * 128 + 128, :].astype(F32)), axis=0, keepdims=True) for n in range(16)])
        scale = lax.rsqrt(squares / 2048.0 + EPS)
        for n in range(16):
            rows = slice(n * 128, n * 128 + 128)
            xnorm[rows, :] = (xall[rows, :].astype(F32) * scale * gaincol[rows, :]).astype(BF16)
        x = xnorm[...]
        qkall[tp, :, 0:128] = dot(x, wq_ref[...], TN).astype(BF16)
        qkall[tp, :, 128:256] = dot(x, wk_ref[...], TN).astype(BF16)
        first = iota((16, 2048), 0) == 0
        wsd = jnp.where(first, jnp.broadcast_to(ws_ref[...].astype(F32), (16, 2048)), jnp.broadcast_to(wd_ref[...].astype(F32), (16, 2048)))
        sdall[tp] = dot(wsd.astype(BF16), x)[0:8]
    stage_c = []
    for d in (2, 1, 3):
        target = (kv, along_chips(d))
        stage_c.append((send(qkall.at[tp], qkall.at[tp], sq.at[d], rq.at[d], target), send(sdall.at[tp], sdall.at[tp], ssd.at[d], rsd.at[d], target)))
    stage_m = [send(qkall.at[tp], qkall.at[tp], sqm.at[0], rqm.at[0], (kv, mate)), send(sdall.at[tp], sdall.at[tp], sdm.at[0], rdm.at[0], (kv, mate))]
    to_mate = send(xnorm, xmate, swm, rwm, (kv, mate))
    with jax.named_scope("wait_w"):
        for c in stage_w:
            c.wait_recv()
    with jax.named_scope("wait_wm"):
        to_mate.wait_recv()
    weights = wvz[...].reshape(128, 2048)
    for h, rows in ((core, xnorm), (1 - core, xmate)):
        product = dot(weights, rows[...]).astype(BF16).reshape(4, 2, 16, 128)
        for n in range(4):
            vzs[n, h] = product[n]
    stage_v = []
    for d in (2, 1, 3):
        stage_v.append(send(vzs.at[lax.rem(chip + d, 4)], vzall.at[chip], svz.at[d], rvz.at[d], (kv, along_chips(d))))
    vzall[chip] = vzs[chip]
    out_tiles = total(xall.at[0:240], so, ro)
    out_tiles.wait_recv()
    block = woall.at[core, chip]
    stage_o = [send(block, block, som.at[d], rom.at[d], (kv, along_chips(d))) for d in (2, 1, 3)]
    stage_o.append(send(block, block, som.at[0], rom.at[0], (kv, mate)))
    with jax.named_scope("wait_c"):
        for d, pair in ((1, stage_c[1]), (3, stage_c[2]), (2, stage_c[0])):
            for c in pair:
                c.wait_recv()
            source = lax.rem(chip + 4 - d, 4) * 2 + core
            stage_m.append(send(qkall.at[source], qkall.at[source], sqm.at[d], rqm.at[d], (kv, mate)))
            stage_m.append(send(sdall.at[source], sdall.at[source], sdm.at[d], rdm.at[d], (kv, mate)))
    with jax.named_scope("wait_v"):
        for c in stage_v:
            c.wait_recv()
    hgain = jnp.broadcast_to(row_to_column(hgain_ref[...].astype(F32)), (16, 128))

    def half(h, offsets):
        lanes = pl.ds(pl.multiple_of(h * 128, 128), 128)

        def query_key(m):
            pieces = [qkall[p * 2 + h, m * 32 : m * 32 + 32, s * 128 : s * 128 + 128] for s in range(2) for p in range(4)]
            return jnp.concatenate(pieces, axis=0)

        outputs = new_part(
            lambda m: abf[pl.ds(pl.multiple_of((h * 4 + m) * 512, 512), 512), :],
            query_key,
            [vzall[p, h, 0].astype(F32) for p in range(4)],
            [sdall[p * 2 + h, 0:1, :] for p in range(4)],
            [sdall[p * 2 + h, 1:2, :] for p in range(4)],
            rate_ref[...],
            [prop_ref[j, :, lanes] for j in range(4)],
            [parent_ref[j : j + 1, lanes] for j in range(4)],
        )
        for p in range(4):
            o, z = outputs[p], vzall[p, h, 1].astype(F32)
            sqs[p * 2 + h] = jnp.sum(jnp.square(o), axis=0, keepdims=True)
            ybuf[p * 2 + h] = (o * hgain * (z * jax.nn.sigmoid(z))).astype(BF16)
        for o in offsets:
            k, t = device(o)
            send(sqs.at[t], sqall.at[own], ses, res, (k, t))
            send(ybuf.at[t], yall.at[core, chip, kv], se, re, (k, t))

    with jax.named_scope("new1"):
        half(core, [o for o in everyone if o[3] == 0])
    sqall[own] = sqs[tp]
    yall[core, chip, kv] = ybuf[tp]
    with jax.named_scope("wait_m"):
        for c in stage_m:
            c.wait_recv()
    with jax.named_scope("new2"):
        half(1 - core, [o for o in everyone if o[3] == 1])
    with jax.named_scope("wait_o"):
        for d, c in ((1, stage_o[1]), (3, stage_o[2]), (2, stage_o[0])):
            c.wait_recv()
            block = woall.at[core, lax.rem(chip + 4 - d, 4)]
            stage_o.append(send(block, block, som.at[3 + d], rom.at[3 + d], (kv, mate)))
        for c in stage_o[3:]:
            c.wait_recv()
    with jax.named_scope("wait_e"):
        all_y, all_sq = total(xall.at[0:2032], se, re), total(sqall.at[0:127], ses, res)
        all_sq.wait_recv()
        all_y.wait_recv()
    with jax.named_scope("combine"):
        for k in range(16):
            scale = lax.rsqrt(sum_of([sqall[k * 8 + t] for t in range(8)]) / 128.0 + EPS)
            for c in range(2):
                for n in range(4):
                    rows = slice(((c * 4 + n) * 16 + k) * 16, ((c * 4 + n) * 16 + k) * 16 + 16)
                    ynorm[rows, :] = (yall[c, n, k].astype(F32) * scale).astype(BF16)
        combined = dot(woall[...].reshape(2048, 128), ynorm[...], TN)
        csend[...] = combined.reshape(8, 16, 128)
        sqf[...] = jnp.sum(jnp.square(combined), axis=0, keepdims=True)
    for o in everyone:
        send(sqf, sums_ref.at[tp * 16 + kv], sh, rh, device(o))
    stage_f = []
    for b, o in enumerate(far_first(itertools.product([0], [0], range(4), range(2)))):
        _, t = device(o)
        stage_f.append(send(csend.at[t], comb_ref.at[tp], sf.at[b], rf.at[b], (kv, t)))
    saves.append(pltpu.make_async_copy(sqf, sums_ref.at[tp * 16 + kv], load_sems.at[0]))
    saves.append(pltpu.make_async_copy(csend.at[tp], comb_ref.at[tp], load_sems.at[1]))
    for c in saves[-2:]:
        c.start()
    sums = total(sqall.at[0:127], sh, rh)
    with jax.named_scope("sends"):
        for pair in stage_c:
            for c in pair:
                c.wait_send()
        for c in stage_w + stage_m + stage_v + stage_o + [to_mate, tokens, out_tiles, all_y, all_sq]:
            c.wait_send()
        for c in saves:
            c.wait()
    with jax.named_scope("wait_f"):
        for c in stage_f:
            c.wait_recv()
    with jax.named_scope("wait_h"):
        sums.wait_recv()
    for c in stage_f + [sums]:
        c.wait_send()


def finish(sums_in, comb_in, gain_in, acc_in, out_ref, acc_ref, sums, comb, gain, outv, accv, loaded, saved):
    pieces = [(sums_in, sums), (comb_in, comb), (gain_in, gain)]
    blocks = [pl.ds(g * 512, 512) for g in range(8)]
    pieces += [(acc_in.at[rows], accv.at[rows]) for rows in blocks]
    loads = [pltpu.make_async_copy(a, b, loaded.at[n]) for n, (a, b) in enumerate(pieces)]
    saves = [pltpu.make_async_copy(accv.at[rows], acc_ref.at[rows], saved.at[g]) for g, rows in enumerate(blocks)]
    saves.append(pltpu.make_async_copy(outv, out_ref, saved.at[8]))
    for c in loads:
        c.start()
    for c in loads[:3]:
        c.wait()
    column = jnp.broadcast_to(row_to_column(gain[...].astype(F32)), (16, 128))
    for t in range(8):
        scale = lax.rsqrt(sum_of([sums[t * 16 + k] for k in range(16)]) / 2048.0 + EPS)
        outv[t // 2, :, (t % 2) * 128 : (t % 2) * 128 + 128] = (comb[t] * scale * column).astype(BF16)
    saves[8].start()
    for load, save in zip(loads[3:], saves):
        load.wait()
        save.start()
    for c in saves:
        c.wait()


def on_device(
    tokens, input_norm_gain, query_weight, key_weight, value_weight, output_gate_weight, strength_weight, decay_weight,
    head_decay_rate, proposal_log_decay, head_norm_gain, output_weight, output_norm_gain, state, previous_keys,
    previous_values, previous_log_decay, previous_strengths, accepted, parent,
):
    tp_n, kv_n = lax.axis_size("tp"), lax.axis_size("kv")
    args = [
        tokens.transpose(1, 2, 0),
        value_weight.transpose(1, 2, 0).reshape(16, 2048),
        output_gate_weight.transpose(1, 2, 0).reshape(16, 2048),
        output_weight.reshape(16, 2048),
        input_norm_gain.reshape(16, 128),
        previous_keys.reshape(1024, 128),
        state.reshape(4096, 128),
        previous_values.transpose(1, 2, 3, 0).reshape(4, 16, 256),
        previous_log_decay.transpose(1, 2, 0),
        previous_strengths.transpose(1, 2, 0),
        accepted.reshape(1, 256),
        query_weight,
        key_weight,
        strength_weight.transpose(1, 0),
        decay_weight.transpose(1, 0),
        head_decay_rate.reshape(1, 1),
        proposal_log_decay.transpose(1, 2, 0),
        parent.transpose(1, 0),
        head_norm_gain.reshape(1, 16),
    ]
    hbm = pl.BlockSpec(memory_space=pltpu.HBM)
    specs = [hbm] * len(args)

    def sems(n):
        return [pltpu.SemaphoreType.DMA((n,)), pltpu.SemaphoreType.DMA((n,))]

    def one():
        return [pltpu.SemaphoreType.DMA(()), pltpu.SemaphoreType.DMA(())]

    sums, combined, acc = pl.pallas_call(
        functools.partial(kernel, tp_n, kv_n),
        out_shape=(
            jax.ShapeDtypeStruct((128, 1, 128), F32),
            jax.ShapeDtypeStruct((8, 16, 128), F32),
            jax.ShapeDtypeStruct((4096, 128), F32),
        ),
        in_specs=specs,
        out_specs=(hbm, hbm, hbm),
        scratch_shapes=[
            *[pltpu.VMEM(a.shape, a.dtype) for a in args],
            pltpu.SemaphoreType.DMA((len(args),)),
            pltpu.VMEM((4096, 128), F32),
            pltpu.SemaphoreType.DMA((8,)),
            pltpu.VMEM((2048, 128), BF16),
            pltpu.VMEM((4, 2, 16, 2048), BF16),
            pltpu.VMEM((2, 4, 16, 16, 128), BF16),
            pltpu.VMEM((2048, 128), F32),
            pltpu.VMEM((2048, 128), BF16),
            pltpu.VMEM((2048, 128), BF16),
            pltpu.VMEM((2048, 128), BF16),
            pltpu.VMEM((8, 128, 256), BF16),
            pltpu.VMEM((4, 2, 2, 16, 128), BF16),
            pltpu.VMEM((4, 2, 2, 16, 128), BF16),
            pltpu.VMEM((8, 8, 128), F32),
            pltpu.VMEM((4096, 128), BF16),
            pltpu.VMEM((8, 16, 128), BF16),
            pltpu.VMEM((2, 4, 16, 16, 128), BF16),
            pltpu.VMEM((8, 1, 128), F32),
            pltpu.VMEM((128, 1, 128), F32),
            pltpu.VMEM((8, 16, 128), F32),
            pltpu.VMEM((1, 128), F32),
            *one(), *sems(8), *one(), *sems(4), *sems(4), *sems(4), *sems(4), *sems(4), *one(), *sems(7), *one(), *one(), *sems(8), *one(),
        ],
        compiler_params=pltpu.CompilerParams(collective_id=0, has_side_effects=True, vmem_limit_bytes=67043328),
    )(*args)
    out, acc = pl.pallas_call(
        finish,
        out_shape=(jax.ShapeDtypeStruct((4, 16, 256), BF16), jax.ShapeDtypeStruct((4096, 128), F32)),
        in_specs=(hbm,) * 4,
        out_specs=(hbm, hbm),
        scratch_shapes=[
            pltpu.VMEM((128, 1, 128), F32),
            pltpu.VMEM((8, 16, 128), F32),
            pltpu.VMEM((1, 16), BF16),
            pltpu.VMEM((4, 16, 256), BF16),
            pltpu.VMEM((4096, 128), F32),
            pltpu.SemaphoreType.DMA((11,)),
            pltpu.SemaphoreType.DMA((9,)),
        ],
        compiler_params=pltpu.CompilerParams(vmem_limit_bytes=67043328),
    )(sums, combined, output_norm_gain.reshape(1, 16), acc)
    return out.transpose(2, 0, 1), acc.reshape(256, 1, 16, 128)


def solution(mesh):
    placed = (
        P(None, None, ("kv", "tp")),
        P(),
        P(None, "kv"),
        P(None, "kv"),
        P(None, "kv", "tp"),
        P(None, "kv", "tp"),
        P(None, "kv"),
        P(None, "kv"),
        P("kv"),
        P(None, None, "kv"),
        P("tp"),
        P("kv", "tp", None),
        P(("kv", "tp")),
        P(None, "kv", "tp", None),
        P(None, None, "kv"),
        P(None, None, "kv", "tp"),
        P(None, None, "kv"),
        P(None, None, "kv"),
        P(),
        P(),
    )
    return jax.shard_map(
        on_device,
        mesh=mesh,
        in_specs=placed,
        out_specs=(P(None, None, ("kv", "tp")), P(None, "kv", "tp", None)),
        check_vma=False,
    )
```

```python
import functools
import itertools

import jax
import jax.numpy as jnp
from jax import lax
from jax.experimental import pallas as pl
from jax.experimental.pallas import tpu as pltpu
from jax.sharding import PartitionSpec as P

EPS = 1e-06
INPUTS = 19
F32 = jnp.float32
BF16 = jnp.bfloat16
MESH = pl.DeviceIdType.MESH
NT = (((1,), (1,)), ((), ()))
NN = (((1,), (0,)), ((), ()))
TN = (((0,), (0,)), ((), ()))


def dot(a, b, dims=NN):
    return lax.dot_general(a, b, dims, preferred_element_type=F32)


def iota(shape, dim):
    return lax.broadcasted_iota(jnp.int32, shape, dim)


def roll(x, shift):
    return x if shift % 128 == 0 else pltpu.roll(x, shift % 128, 1)


def row_to_column(row):
    n = row.shape[1]
    square = jnp.broadcast_to(row, (n, n))
    return jnp.sum(jnp.where(iota((n, n), 0) == iota((n, n), 1), square, 0.0), axis=1, keepdims=True)


def ungroup_half(parts, j):
    chunk = iota(parts[0].shape, 1) // 32
    total = parts[0] if j == 0 else roll(parts[0], -j * 32)
    for m in range(1, 4):
        total = jnp.where(chunk == m, roll(parts[m], (m - j) * 32), total)
    return total


def ungroup(parts, j):
    return jnp.concatenate([ungroup_half(parts[:4], j), ungroup_half(parts[4:], j)], axis=1)


def regroup(rows, g):
    h, m = divmod(g, 4)
    total = None
    for j in range(4):
        x = roll(rows[j][:, h * 128 : h * 128 + 128], (j - m) * 32)
        total = x if total is None else jnp.where(iota(x.shape, 1) // 32 == j, x, total)
    return total


def pick_rows(product):
    lanes = product.shape[1]
    cube = product.reshape(32, 16, lanes)
    keep = iota(cube.shape, 0) == iota(cube.shape, 2) % 32
    return jnp.sum(jnp.where(keep, cube, 0.0), axis=0)


def pick_pairs(product):
    n, lanes = product.shape[0] // 32, product.shape[1]
    cube = product.reshape(n, 32, lanes)
    keep = iota(cube.shape, 1) == iota(cube.shape, 2) % 32
    return jnp.sum(jnp.where(keep, cube, 0.0), axis=1)


def sum_of(terms):
    return functools.reduce(lambda a, b: a + b, terms)


def far_first(offsets):
    return sorted([o for o in offsets if any(o)], key=lambda o: -sum(min(d, 4 - d) for d in o[:3]))


def old_part(state, keys, old_values, log_decay, strengths, accepted, store):
    source, target = iota((128, 128), 1), iota((128, 128), 0)
    order = (source == (target % 32) * 4 + target // 32).astype(BF16)
    grouped, reads, grams = [], [], []
    for g in range(8):
        kg = dot(order, keys(g)).astype(BF16)
        grouped.append(kg)
        reads.append(pick_rows(dot(state(g).astype(BF16), kg, NT)))
        grams.append(pick_pairs(dot(kg, kg, NT)))
    gram = [ungroup(grams, j) for j in range(4)]
    read = [ungroup(reads, j) for j in range(4)]
    inv = [lax.rsqrt(gram[j][j : j + 1] + EPS) for j in range(4)]
    gam, beta = [], []
    for j in range(4):
        live = (j < accepted).astype(F32)
        g_j = log_decay[j] * live
        gam.append(g_j if j == 0 else gam[-1] + g_j)
        beta.append(strengths[j] * live)
    update = []
    for i in range(4):
        u = beta[i] * (old_values[i] - (jnp.exp(gam[i]) * inv[i]) * read[i])
        for j in range(i):
            a = beta[i] * (gram[j][i : i + 1] * (inv[i] * inv[j])) * jnp.exp(gam[i] - gam[j])
            u = u - a * update[j]
        update.append(u)
    weighted = [update[j] * (jnp.exp(gam[3] - gam[j]) * inv[j]) for j in range(4)]
    kept = jnp.exp(gam[3])
    columns = [jnp.broadcast_to(row_to_column(kept[:, h * 128 : h * 128 + 128]), (128, 128)) for h in range(2)]
    for g in range(8):
        wg = regroup(weighted, g)
        cube = (32, 16, 128)
        keep = iota(cube, 0) == iota(cube, 2) % 32
        block = jnp.where(keep, jnp.broadcast_to(wg[None], cube), 0.0).reshape(512, 128).astype(BF16)
        h, m = divmod(g, 4)
        scale = jnp.broadcast_to(columns[h][m * 32 : m * 32 + 32][:, None, :], cube).reshape(512, 128)
        store(g, scale * state(g) + dot(block, grouped[g]))


def new_reads(accepted_state, query_key):
    reads, grams = [], []
    for m in range(4):
        qk = query_key(m)
        reads.append(pick_rows(dot(accepted_state(m), qk, NT)))
        grams.append(pick_pairs(dot(qk, qk, NT)))
    aq = [ungroup_half([r[:, :128] for r in reads], j) for j in range(4)]
    ak = [ungroup_half([r[:, 128:] for r in reads], j) for j in range(4)]
    gq = [ungroup_half([r[:, :128] for r in grams], j) for j in range(4)]
    gk = [ungroup_half([r[:, 128:] for r in grams], j) for j in range(4)]
    inv_q = [lax.rsqrt(gq[j][j : j + 1] + EPS) * (128.0**-0.5) for j in range(4)]
    inv_k = [lax.rsqrt(gk[j][4 + j : 5 + j] + EPS) for j in range(4)]
    return aq, ak, gk, inv_q, inv_k


def new_part(products, values, beta_pre, decay_pre, rate, proposal, parent):
    aq, ak, gk, inv_q, inv_k = products
    ancestors = []
    for i in range(4):
        row = {j: (parent[i] == j).astype(F32) for j in range(i)}
        row = {j: row[j] + sum_of([jnp.zeros_like(row[j])] + [row[m] * ancestors[m][j] for m in range(j + 1, i)]) for j in range(i)}
        ancestors.append(row)
    beta, g_new, gam = [], [], []
    for i in range(4):
        x = decay_pre[i]
        softplus = jnp.maximum(x, 0.0) + jnp.log1p(jnp.exp(-jnp.abs(x)))
        g_new.append(-rate * softplus + proposal[i])
        beta.append(jax.nn.sigmoid(beta_pre[i]))
        gam.append(sum_of([g_new[i]] + [ancestors[i][j] * g_new[j] for j in range(i)]))
    outputs, update = [], []
    for i in range(4):
        grow = jnp.exp(gam[i])
        u = beta[i] * (values[i] - (grow * inv_k[i]) * ak[i])
        o = (grow * inv_q[i]) * aq[i]
        for j in range(i):
            reach = jnp.exp(jnp.minimum(gam[i] - gam[j], 0.0)) * ancestors[i][j] * inv_k[j]
            u = u - (beta[i] * inv_k[i] * gk[j][4 + i : 5 + i] * reach) * update[j]
            o = o + (inv_q[i] * gk[j][i : i + 1] * reach) * update[j]
        update.append(u)
        o = o + (inv_q[i] * gk[i][i : i + 1] * inv_k[i]) * u
        outputs.append(o)
    return outputs


def kernel(
    tp_n, kv_n, *refs,
):
    run(tp_n, kv_n, refs[:INPUTS], *refs[INPUTS:])


def run(
    tp_n, kv_n, sources, sums_ref, comb_ref, acc_ref,
    xt_ref, wv_ref, wz_ref, wo_ref, gain_ref, keys_ref, state_ref, oldv_ref, logd_ref, strength_ref, accepted_ref,
    wq_ref, wk_ref, ws_ref, wd_ref, rate_ref, prop_ref, parent_ref, hgain_ref,
    load_sems, accv, acc_sems,
    xall, wvz, woall, gaincol, xnorm, xmate, ynorm, qkall, vzs, vzall, sdall, abf, ybuf, yall, sqs, sqall, csend, sqf,
    sa, ra, st, rt, sv, rv, swm, rwm, sq, rq, ssd, rsd, sqm, rqm, sdm, rdm, svz, rvz, so, ro, som, rom, se, re, ses, res, sf, rf, sh, rh,
):
    held = (
        xt_ref, wv_ref, wz_ref, wo_ref, gain_ref, keys_ref, state_ref, oldv_ref, logd_ref, strength_ref, accepted_ref,
        wq_ref, wk_ref, ws_ref, wd_ref, rate_ref, prop_ref, parent_ref, hgain_ref,
    )
    loads = [pltpu.make_async_copy(src, dst, load_sems.at[n]) for n, (src, dst) in enumerate(zip(sources, held))]
    kv, tp = lax.axis_index("kv"), lax.axis_index("tp")
    chip, core = tp // 2, lax.rem(tp, 2)
    mate = tp + 1 - 2 * core
    own = kv * tp_n + tp
    everyone = far_first(itertools.product(range(4), range(4), range(4), range(2)))
    high, low = kv // 4, lax.rem(kv, 4)

    def device(offset):
        z, y, x, c = offset
        return lax.rem(high + z, 4) * 4 + lax.rem(low + y, 4), lax.rem(chip + x, 4) * 2 + lax.rem(core + c, 2)

    def send(src, dst, send_sem, recv_sem, target):
        c = remote(src, dst, send_sem, recv_sem, target)
        c.start()
        return c

    def remote(src, dst, send_sem, recv_sem, target):
        return pltpu.make_async_remote_copy(
            src_ref=src, dst_ref=dst, send_sem=send_sem, recv_sem=recv_sem, device_id=target, device_id_type=MESH
        )

    def total(ref, send_sem, recv_sem):
        return remote(ref, ref, send_sem, recv_sem, (kv, mate))

    def along_chips(d):
        return lax.rem(chip + d, 4) * 2 + core

    def lanes_of(t):
        return pl.ds(pl.multiple_of(lax.rem(t, 2) * 128, 128), 128)

    barrier = pltpu.get_barrier_semaphore()
    for c in loads[:5]:
        c.start()
    plane = far_first(itertools.product(range(4), range(4), [0], [0]))
    line = far_first(itertools.product([0], [0], range(4), range(2)))
    for o in plane + line:
        pl.semaphore_signal(barrier, inc=1, device_id=device(o), device_id_type=MESH)
    for c in loads[5:]:
        c.start()
    for c in loads[:5]:
        c.wait()
    with jax.named_scope("barrier"):
        pl.semaphore_wait(barrier, kv_n - 1 + tp_n - 1)

    def hand_on(first, count):
        rows = pl.ds(pl.multiple_of((kv * tp_n + first) * 16, 16), count * 16)
        for o in plane:
            send(xall.at[rows], xall.at[rows], st, rt, device(o))

    own_rows = pl.ds(pl.multiple_of(own * 16, 16), 16)
    stage_a = {}
    with jax.named_scope("issue_t"):
        for b, o in enumerate(line):
            _, t = device(o)
            stage_a[o[2:]] = send(xt_ref.at[t // 2, :, lanes_of(t)], xall.at[own_rows], sa.at[b], ra.at[b], (kv, t))
        xall[own_rows, :] = xt_ref[tp // 2, :, lanes_of(tp)]
        own_tile = xt_ref.at[tp // 2, :, lanes_of(tp)]
        for o in plane:
            send(own_tile, xall.at[own_rows], st, rt, device(o))

    stage_w = []
    for d in (2, 1, 3):
        target = (kv, along_chips(d))
        stage_w.append(send(wv_ref, wvz.at[chip, 0], sv.at[d], rv.at[d], target))
        stage_w.append(send(wz_ref, wvz.at[chip, 1], sv.at[4 + d], rv.at[4 + d], target))
    wvz[chip, 0] = wv_ref[...]
    wvz[chip, 1] = wz_ref[...]
    for o in plane:
        k, _ = device(o)
        cols = pl.ds(pl.multiple_of(k * 128, 128), 128)
        send(wo_ref.at[:, cols], woall.at[core, chip, kv], so, ro, (k, tp))
    woall[core, chip, kv] = wo_ref[:, pl.ds(pl.multiple_of(kv * 128, 128), 128)]
    for n in range(16):
        column = row_to_column(gain_ref[n : n + 1, :].astype(F32))
        gaincol[n * 128 : n * 128 + 128, :] = jnp.broadcast_to(column, (128, 128))
    with jax.named_scope("wait_a"):
        stage_a[0, 1].wait_recv()
        hand_on(mate, 1)
        for d in (1, 3, 2):
            for c in range(2):
                stage_a[d, c].wait_recv()
            hand_on(lax.rem(chip + 4 - d, 4) * 2, 2)
    tokens = total(xall.at[0:1920], st, rt)
    for c in loads[5:]:
        c.wait()

    saves = []

    def store(g, value):
        rows = slice(g * 512, g * 512 + 512)
        accv[rows, :] = value
        saves.append(pltpu.make_async_copy(accv.at[rows], acc_ref.at[rows], acc_sems.at[g]))
        saves[-1].start()
        abf[g * 512 : g * 512 + 512, :] = value.astype(BF16)

    with jax.named_scope("old"):
        old_part(
            lambda g: state_ref[g * 512 : g * 512 + 512, :],
            lambda g: keys_ref[g * 128 : g * 128 + 128, :],
            [oldv_ref[j].astype(F32) for j in range(4)],
            [logd_ref[j] for j in range(4)],
            [strength_ref[j] for j in range(4)],
            accepted_ref[...],
            store,
        )

    out_tiles = total(xall.at[0:240], so, ro)
    out_tiles.wait_recv()
    block = woall.at[core, chip]
    stage_o = [send(block, block, som.at[d], rom.at[d], (kv, along_chips(d))) for d in (2, 1, 3)]
    stage_o.append(send(block, block, som.at[0], rom.at[0], (kv, mate)))
    with jax.named_scope("wait_t"):
        tokens.wait_recv()
    with jax.named_scope("project"):
        squares = sum_of([jnp.sum(jnp.square(xall[n * 128 : n * 128 + 128, :].astype(F32)), axis=0, keepdims=True) for n in range(16)])
        scale = lax.rsqrt(squares / 2048.0 + EPS)
        for n in range(16):
            rows = slice(n * 128, n * 128 + 128)
            xnorm[rows, :] = (xall[rows, :].astype(F32) * scale * gaincol[rows, :]).astype(BF16)
        x = xnorm[...]
        qkall[tp, :, 0:128] = dot(x, wq_ref[...], TN).astype(BF16)
        qkall[tp, :, 128:256] = dot(x, wk_ref[...], TN).astype(BF16)
        first = iota((16, 2048), 0) == 0
        wsd = jnp.where(first, jnp.broadcast_to(ws_ref[...].astype(F32), (16, 2048)), jnp.broadcast_to(wd_ref[...].astype(F32), (16, 2048)))
        sdall[tp] = dot(wsd.astype(BF16), x)[0:8]
    stage_c = []
    for d in (2, 1, 3):
        target = (kv, along_chips(d))
        stage_c.append((send(qkall.at[tp], qkall.at[tp], sq.at[d], rq.at[d], target), send(sdall.at[tp], sdall.at[tp], ssd.at[d], rsd.at[d], target)))
    stage_m = [send(qkall.at[tp], qkall.at[tp], sqm.at[0], rqm.at[0], (kv, mate)), send(sdall.at[tp], sdall.at[tp], sdm.at[0], rdm.at[0], (kv, mate))]
    to_mate = send(xnorm, xmate, swm, rwm, (kv, mate))
    with jax.named_scope("wait_w"):
        for c in stage_w:
            c.wait_recv()
    with jax.named_scope("wait_wm"):
        to_mate.wait_recv()
    weights = wvz[...].reshape(128, 2048)
    for h, rows in ((core, xnorm), (1 - core, xmate)):
        product = dot(weights, rows[...]).astype(BF16).reshape(4, 2, 16, 128)
        for n in range(4):
            vzs[n, h] = product[n]
    stage_v = []
    for d in (2, 1, 3):
        stage_v.append(send(vzs.at[lax.rem(chip + d, 4)], vzall.at[chip], svz.at[d], rvz.at[d], (kv, along_chips(d))))
    vzall[chip] = vzs[chip]
    with jax.named_scope("wait_c"):
        for d, pair in ((1, stage_c[1]), (3, stage_c[2]), (2, stage_c[0])):
            for c in pair:
                c.wait_recv()
            source = lax.rem(chip + 4 - d, 4) * 2 + core
            stage_m.append(send(qkall.at[source], qkall.at[source], sqm.at[d], rqm.at[d], (kv, mate)))
            stage_m.append(send(sdall.at[source], sdall.at[source], sdm.at[d], rdm.at[d], (kv, mate)))
    hgain = jnp.broadcast_to(row_to_column(hgain_ref[...].astype(F32)), (16, 128))

    def reads_of(h):
        def query_key(m):
            pieces = [qkall[p * 2 + h, m * 32 : m * 32 + 32, s * 128 : s * 128 + 128] for s in range(2) for p in range(4)]
            return jnp.concatenate(pieces, axis=0)

        return new_reads(lambda m: abf[pl.ds(pl.multiple_of((h * 4 + m) * 512, 512), 512), :], query_key)

    def half(h, products, offsets):
        lanes = pl.ds(pl.multiple_of(h * 128, 128), 128)
        outputs = new_part(
            products,
            [vzall[p, h, 0].astype(F32) for p in range(4)],
            [sdall[p * 2 + h, 0:1, :] for p in range(4)],
            [sdall[p * 2 + h, 1:2, :] for p in range(4)],
            rate_ref[...],
            [prop_ref[j, :, lanes] for j in range(4)],
            [parent_ref[j : j + 1, lanes] for j in range(4)],
        )
        for p in range(4):
            o, z = outputs[p], vzall[p, h, 1].astype(F32)
            sqs[p * 2 + h] = jnp.sum(jnp.square(o), axis=0, keepdims=True)
            ybuf[p * 2 + h] = (o * hgain * (z * jax.nn.sigmoid(z))).astype(BF16)
        for o in offsets:
            k, t = device(o)
            send(sqs.at[t], sqall.at[own], ses, res, (k, t))
            send(ybuf.at[t], yall.at[core, chip, kv], se, re, (k, t))

    with jax.named_scope("reads1"):
        products = reads_of(core)
    with jax.named_scope("wait_v"):
        for c in stage_v:
            c.wait_recv()
    with jax.named_scope("new1"):
        half(core, products, [o for o in everyone if o[3] == 0])
    sqall[own] = sqs[tp]
    yall[core, chip, kv] = ybuf[tp]
    with jax.named_scope("wait_m"):
        for c in stage_m:
            c.wait_recv()
    with jax.named_scope("new2"):
        half(1 - core, reads_of(1 - core), [o for o in everyone if o[3] == 1])
    with jax.named_scope("wait_o"):
        for d, c in ((1, stage_o[1]), (3, stage_o[2]), (2, stage_o[0])):
            c.wait_recv()
            block = woall.at[core, lax.rem(chip + 4 - d, 4)]
            stage_o.append(send(block, block, som.at[3 + d], rom.at[3 + d], (kv, mate)))
        for c in stage_o[3:]:
            c.wait_recv()
    with jax.named_scope("wait_e"):
        all_y, all_sq = total(xall.at[0:2032], se, re), total(sqall.at[0:127], ses, res)
        all_sq.wait_recv()
        all_y.wait_recv()
    with jax.named_scope("combine"):
        for k in range(16):
            scale = lax.rsqrt(sum_of([sqall[k * 8 + t] for t in range(8)]) / 128.0 + EPS)
            for c in range(2):
                for n in range(4):
                    rows = slice(((c * 4 + n) * 16 + k) * 16, ((c * 4 + n) * 16 + k) * 16 + 16)
                    ynorm[rows, :] = (yall[c, n, k].astype(F32) * scale).astype(BF16)
        combined = dot(woall[...].reshape(2048, 128), ynorm[...], TN)
        csend[...] = combined.reshape(8, 16, 128)
        sqf[...] = jnp.sum(jnp.square(combined), axis=0, keepdims=True)
    for o in everyone:
        send(sqf, sums_ref.at[tp * 16 + kv], sh, rh, device(o))
    stage_f = []
    for b, o in enumerate(line):
        _, t = device(o)
        stage_f.append(send(csend.at[t], comb_ref.at[tp], sf.at[b], rf.at[b], (kv, t)))
    saves.append(pltpu.make_async_copy(sqf, sums_ref.at[tp * 16 + kv], load_sems.at[0]))
    saves.append(pltpu.make_async_copy(csend.at[tp], comb_ref.at[tp], load_sems.at[1]))
    for c in saves[-2:]:
        c.start()
    sums = total(sqall.at[0:127], sh, rh)
    with jax.named_scope("sends"):
        for pair in stage_c:
            for c in pair:
                c.wait_send()
        for c in list(stage_a.values()) + stage_w + stage_m + stage_v + stage_o + [to_mate, tokens, out_tiles, all_y, all_sq]:
            c.wait_send()
        for c in saves:
            c.wait()
    with jax.named_scope("wait_f"):
        for c in stage_f:
            c.wait_recv()
    with jax.named_scope("wait_h"):
        sums.wait_recv()
    for c in stage_f + [sums]:
        c.wait_send()


def finish(sums_in, comb_in, gain_in, acc_in, out_ref, acc_ref, sums, comb, gain, outv, accv, loaded, saved):
    pieces = [(sums_in, sums), (comb_in, comb), (gain_in, gain)]
    blocks = [pl.ds(g * 512, 512) for g in range(8)]
    pieces += [(acc_in.at[rows], accv.at[rows]) for rows in blocks]
    loads = [pltpu.make_async_copy(a, b, loaded.at[n]) for n, (a, b) in enumerate(pieces)]
    saves = [pltpu.make_async_copy(accv.at[rows], acc_ref.at[rows], saved.at[g]) for g, rows in enumerate(blocks)]
    saves.append(pltpu.make_async_copy(outv, out_ref, saved.at[8]))
    for c in loads:
        c.start()
    for c in loads[:3]:
        c.wait()
    column = jnp.broadcast_to(row_to_column(gain[...].astype(F32)), (16, 128))
    for t in range(8):
        scale = lax.rsqrt(sum_of([sums[t * 16 + k] for k in range(16)]) / 2048.0 + EPS)
        outv[t // 2, :, (t % 2) * 128 : (t % 2) * 128 + 128] = (comb[t] * scale * column).astype(BF16)
    saves[8].start()
    for load, save in zip(loads[3:], saves):
        load.wait()
        save.start()
    for c in saves:
        c.wait()


def on_device(
    tokens, input_norm_gain, query_weight, key_weight, value_weight, output_gate_weight, strength_weight, decay_weight,
    head_decay_rate, proposal_log_decay, head_norm_gain, output_weight, output_norm_gain, state, previous_keys,
    previous_values, previous_log_decay, previous_strengths, accepted, parent,
):
    tp_n, kv_n = lax.axis_size("tp"), lax.axis_size("kv")
    args = [
        tokens.transpose(1, 2, 0),
        value_weight.transpose(1, 2, 0).reshape(16, 2048),
        output_gate_weight.transpose(1, 2, 0).reshape(16, 2048),
        output_weight.reshape(16, 2048),
        input_norm_gain.reshape(16, 128),
        previous_keys.reshape(1024, 128),
        state.reshape(4096, 128),
        previous_values.transpose(1, 2, 3, 0).reshape(4, 16, 256),
        previous_log_decay.transpose(1, 2, 0),
        previous_strengths.transpose(1, 2, 0),
        accepted.reshape(1, 256),
        query_weight,
        key_weight,
        strength_weight.transpose(1, 0),
        decay_weight.transpose(1, 0),
        head_decay_rate.reshape(1, 1),
        proposal_log_decay.transpose(1, 2, 0),
        parent.transpose(1, 0),
        head_norm_gain.reshape(1, 16),
    ]
    hbm = pl.BlockSpec(memory_space=pltpu.HBM)
    specs = [hbm] * len(args)

    def sems(n):
        return [pltpu.SemaphoreType.DMA((n,)), pltpu.SemaphoreType.DMA((n,))]

    def one():
        return [pltpu.SemaphoreType.DMA(()), pltpu.SemaphoreType.DMA(())]

    sums, combined, acc = pl.pallas_call(
        functools.partial(kernel, tp_n, kv_n),
        out_shape=(
            jax.ShapeDtypeStruct((128, 1, 128), F32),
            jax.ShapeDtypeStruct((8, 16, 128), F32),
            jax.ShapeDtypeStruct((4096, 128), F32),
        ),
        in_specs=specs,
        out_specs=(hbm, hbm, hbm),
        scratch_shapes=[
            *[pltpu.VMEM(a.shape, a.dtype) for a in args],
            pltpu.SemaphoreType.DMA((len(args),)),
            pltpu.VMEM((4096, 128), F32),
            pltpu.SemaphoreType.DMA((8,)),
            pltpu.VMEM((2048, 128), BF16),
            pltpu.VMEM((4, 2, 16, 2048), BF16),
            pltpu.VMEM((2, 4, 16, 16, 128), BF16),
            pltpu.VMEM((2048, 128), F32),
            pltpu.VMEM((2048, 128), BF16),
            pltpu.VMEM((2048, 128), BF16),
            pltpu.VMEM((2048, 128), BF16),
            pltpu.VMEM((8, 128, 256), BF16),
            pltpu.VMEM((4, 2, 2, 16, 128), BF16),
            pltpu.VMEM((4, 2, 2, 16, 128), BF16),
            pltpu.VMEM((8, 8, 128), F32),
            pltpu.VMEM((4096, 128), BF16),
            pltpu.VMEM((8, 16, 128), BF16),
            pltpu.VMEM((2, 4, 16, 16, 128), BF16),
            pltpu.VMEM((8, 1, 128), F32),
            pltpu.VMEM((128, 1, 128), F32),
            pltpu.VMEM((8, 16, 128), F32),
            pltpu.VMEM((1, 128), F32),
            *sems(8), *one(), *sems(8), *one(), *sems(4), *sems(4), *sems(4), *sems(4), *sems(4), *one(), *sems(7), *one(), *one(), *sems(8), *one(),
        ],
        compiler_params=pltpu.CompilerParams(collective_id=0, has_side_effects=True, vmem_limit_bytes=67043328),
    )(*args)
    out, acc = pl.pallas_call(
        finish,
        out_shape=(jax.ShapeDtypeStruct((4, 16, 256), BF16), jax.ShapeDtypeStruct((4096, 128), F32)),
        in_specs=(hbm,) * 4,
        out_specs=(hbm, hbm),
        scratch_shapes=[
            pltpu.VMEM((128, 1, 128), F32),
            pltpu.VMEM((8, 16, 128), F32),
            pltpu.VMEM((1, 16), BF16),
            pltpu.VMEM((4, 16, 256), BF16),
            pltpu.VMEM((4096, 128), F32),
            pltpu.SemaphoreType.DMA((11,)),
            pltpu.SemaphoreType.DMA((9,)),
        ],
        compiler_params=pltpu.CompilerParams(vmem_limit_bytes=67043328),
    )(sums, combined, output_norm_gain.reshape(1, 16), acc)
    return out.transpose(2, 0, 1), acc.reshape(256, 1, 16, 128)


def solution(mesh):
    placed = (
        P(None, None, ("kv", "tp")),
        P(),
        P(None, "kv"),
        P(None, "kv"),
        P(None, "kv", "tp"),
        P(None, "kv", "tp"),
        P(None, "kv"),
        P(None, "kv"),
        P("kv"),
        P(None, None, "kv"),
        P("tp"),
        P("kv", "tp", None),
        P(("kv", "tp")),
        P(None, "kv", "tp", None),
        P(None, None, "kv"),
        P(None, None, "kv", "tp"),
        P(None, None, "kv"),
        P(None, None, "kv"),
        P(),
        P(),
    )
    return jax.shard_map(
        on_device,
        mesh=mesh,
        in_specs=placed,
        out_specs=(P(None, None, ("kv", "tp")), P(None, "kv", "tp", None)),
        check_vma=False,
    )
```

```python
import functools
import itertools

import jax
import jax.numpy as jnp
from jax import lax
from jax.experimental import pallas as pl
from jax.experimental.pallas import tpu as pltpu
from jax.sharding import PartitionSpec as P

EPS = 1e-06
INPUTS = 19
F32 = jnp.float32
BF16 = jnp.bfloat16
MESH = pl.DeviceIdType.MESH
NT = (((1,), (1,)), ((), ()))
NN = (((1,), (0,)), ((), ()))
TN = (((0,), (0,)), ((), ()))


def dot(a, b, dims=NN):
    return lax.dot_general(a, b, dims, preferred_element_type=F32)


def iota(shape, dim):
    return lax.broadcasted_iota(jnp.int32, shape, dim)


def roll(x, shift):
    return x if shift % 128 == 0 else pltpu.roll(x, shift % 128, 1)


def row_to_column(row):
    n = row.shape[1]
    square = jnp.broadcast_to(row, (n, n))
    return jnp.sum(jnp.where(iota((n, n), 0) == iota((n, n), 1), square, 0.0), axis=1, keepdims=True)


def ungroup_half(parts, j):
    chunk = iota(parts[0].shape, 1) // 32
    total = parts[0] if j == 0 else roll(parts[0], -j * 32)
    for m in range(1, 4):
        total = jnp.where(chunk == m, roll(parts[m], (m - j) * 32), total)
    return total


def ungroup(parts, j):
    return jnp.concatenate([ungroup_half(parts[:4], j), ungroup_half(parts[4:], j)], axis=1)


def regroup(rows, g):
    h, m = divmod(g, 4)
    total = None
    for j in range(4):
        x = roll(rows[j][:, h * 128 : h * 128 + 128], (j - m) * 32)
        total = x if total is None else jnp.where(iota(x.shape, 1) // 32 == j, x, total)
    return total


def pick_rows(product):
    lanes = product.shape[1]
    cube = product.reshape(32, 16, lanes)
    keep = iota(cube.shape, 0) == iota(cube.shape, 2) % 32
    return jnp.sum(jnp.where(keep, cube, 0.0), axis=0)


def pick_pairs(product):
    n, lanes = product.shape[0] // 32, product.shape[1]
    cube = product.reshape(n, 32, lanes)
    keep = iota(cube.shape, 1) == iota(cube.shape, 2) % 32
    return jnp.sum(jnp.where(keep, cube, 0.0), axis=1)


def sum_of(terms):
    return functools.reduce(lambda a, b: a + b, terms)


def far_first(offsets):
    return sorted([o for o in offsets if any(o)], key=lambda o: -sum(min(d, 4 - d) for d in o[:3]))


def old_part(state, keys, old_values, log_decay, strengths, accepted, store):
    source, target = iota((128, 128), 1), iota((128, 128), 0)
    order = (source == (target % 32) * 4 + target // 32).astype(BF16)
    grouped, reads, grams = [], [], []
    for g in range(8):
        kg = dot(order, keys(g)).astype(BF16)
        grouped.append(kg)
        reads.append(pick_rows(dot(state(g).astype(BF16), kg, NT)))
        grams.append(pick_pairs(dot(kg, kg, NT)))
    gram = [ungroup(grams, j) for j in range(4)]
    read = [ungroup(reads, j) for j in range(4)]
    inv = [lax.rsqrt(gram[j][j : j + 1] + EPS) for j in range(4)]
    gam, beta = [], []
    for j in range(4):
        live = (j < accepted).astype(F32)
        g_j = log_decay[j] * live
        gam.append(g_j if j == 0 else gam[-1] + g_j)
        beta.append(strengths[j] * live)
    update = []
    for i in range(4):
        u = beta[i] * (old_values[i] - (jnp.exp(gam[i]) * inv[i]) * read[i])
        for j in range(i):
            a = beta[i] * (gram[j][i : i + 1] * (inv[i] * inv[j])) * jnp.exp(gam[i] - gam[j])
            u = u - a * update[j]
        update.append(u)
    weighted = [update[j] * (jnp.exp(gam[3] - gam[j]) * inv[j]) for j in range(4)]
    kept = jnp.exp(gam[3])
    columns = [jnp.broadcast_to(row_to_column(kept[:, h * 128 : h * 128 + 128]), (128, 128)) for h in range(2)]
    for g in range(8):
        wg = regroup(weighted, g)
        cube = (32, 16, 128)
        keep = iota(cube, 0) == iota(cube, 2) % 32
        block = jnp.where(keep, jnp.broadcast_to(wg[None], cube), 0.0).reshape(512, 128).astype(BF16)
        h, m = divmod(g, 4)
        scale = jnp.broadcast_to(columns[h][m * 32 : m * 32 + 32][:, None, :], cube).reshape(512, 128)
        store(g, scale * state(g) + dot(block, grouped[g]))


def new_reads(accepted_state, query_key):
    reads, grams = ([], []), []
    for m in range(4):
        qk = query_key(m)
        for c, state in enumerate(accepted_state(m)):
            reads[c].append(pick_rows(dot(state, qk, NT)))
        grams.append(pick_pairs(dot(qk, qk, NT)))
    aq = [[ungroup_half([r[:, :128] for r in reads[c]], j) for j in range(4)] for c in range(2)]
    ak = [[ungroup_half([r[:, 128:] for r in reads[c]], j) for j in range(4)] for c in range(2)]
    gq = [ungroup_half([r[:, :128] for r in grams], j) for j in range(4)]
    gk = [ungroup_half([r[:, 128:] for r in grams], j) for j in range(4)]
    inv_q = [lax.rsqrt(gq[j][j : j + 1] + EPS) * (128.0**-0.5) for j in range(4)]
    inv_k = [lax.rsqrt(gk[j][4 + j : 5 + j] + EPS) for j in range(4)]
    return aq, ak, gk, inv_q, inv_k


def new_part(products, values, beta_pre, decay_pre, rate, proposal, parent):
    aq, ak, gk, inv_q, inv_k = products
    ancestors = []
    for i in range(4):
        row = {j: (parent[i] == j).astype(F32) for j in range(i)}
        row = {j: row[j] + sum_of([jnp.zeros_like(row[j])] + [row[m] * ancestors[m][j] for m in range(j + 1, i)]) for j in range(i)}
        ancestors.append(row)
    beta, g_new, gam = [], [], []
    for i in range(4):
        x = decay_pre[i]
        softplus = jnp.maximum(x, 0.0) + jnp.log1p(jnp.exp(-jnp.abs(x)))
        g_new.append(-rate * softplus + proposal[i])
        beta.append(jax.nn.sigmoid(beta_pre[i]))
        gam.append(sum_of([g_new[i]] + [ancestors[i][j] * g_new[j] for j in range(i)]))
    outputs, update = ([], []), ([], [])
    for i in range(4):
        grow = jnp.exp(gam[i])
        reach = [jnp.exp(jnp.minimum(gam[i] - gam[j], 0.0)) * ancestors[i][j] * inv_k[j] for j in range(i)]
        for c in range(2):
            u = beta[i] * (values[c][i] - (grow * inv_k[i]) * ak[c][i])
            o = (grow * inv_q[i]) * aq[c][i]
            for j in range(i):
                u = u - (beta[i] * inv_k[i] * gk[j][4 + i : 5 + i] * reach[j]) * update[c][j]
                o = o + (inv_q[i] * gk[j][i : i + 1] * reach[j]) * update[c][j]
            update[c].append(u)
            outputs[c].append(o + (inv_q[i] * gk[i][i : i + 1] * inv_k[i]) * u)
    return outputs


def kernel(
    tp_n, kv_n, *refs,
):
    run(tp_n, kv_n, refs[:INPUTS], *refs[INPUTS:])


def run(
    tp_n, kv_n, sources, sums_ref, comb_ref, acc_ref,
    xt_ref, wv_ref, wz_ref, wo_ref, gain_ref, keys_ref, state_ref, oldv_ref, logd_ref, strength_ref, accepted_ref,
    wq_ref, wk_ref, ws_ref, wd_ref, rate_ref, prop_ref, parent_ref, hgain_ref,
    load_sems, accv, acc_sem,
    xall, wvz, woall, gaincol, hgcol, xnorm, ynorm, qkall, vzs, vzall, sdall, abf, amate, ybuf, yall, sqs, sqall, csend, sqf,
    sa, ra, st, rt, sv, rv, swm, rwm, sq, rq, svz, rvz, so, ro, som, rom, se, re, ses, res, sf, rf, sh, rh,
):
    held = (
        xt_ref, wv_ref, wz_ref, wo_ref, gain_ref, keys_ref, state_ref, oldv_ref, logd_ref, strength_ref, accepted_ref,
        wq_ref, wk_ref, ws_ref, wd_ref, rate_ref, prop_ref, parent_ref, hgain_ref,
    )
    loads = [pltpu.make_async_copy(src, dst, load_sems.at[n]) for n, (src, dst) in enumerate(zip(sources, held))]
    kv, tp = lax.axis_index("kv"), lax.axis_index("tp")
    chip, core = tp // 2, lax.rem(tp, 2)
    mate = tp + 1 - 2 * core
    own = kv * tp_n + tp
    everyone = far_first(itertools.product(range(4), range(4), range(4), range(2)))
    high, low = kv // 4, lax.rem(kv, 4)

    def device(offset):
        z, y, x, c = offset
        return lax.rem(high + z, 4) * 4 + lax.rem(low + y, 4), lax.rem(chip + x, 4) * 2 + lax.rem(core + c, 2)

    def send(src, dst, send_sem, recv_sem, target):
        c = remote(src, dst, send_sem, recv_sem, target)
        c.start()
        return c

    def remote(src, dst, send_sem, recv_sem, target):
        return pltpu.make_async_remote_copy(
            src_ref=src, dst_ref=dst, send_sem=send_sem, recv_sem=recv_sem, device_id=target, device_id_type=MESH
        )

    def total(ref, send_sem, recv_sem):
        return remote(ref, ref, send_sem, recv_sem, (kv, mate))

    def along_chips(d):
        return lax.rem(chip + d, 4) * 2 + core

    def lanes_of(t):
        return pl.ds(pl.multiple_of(lax.rem(t, 2) * 128, 128), 128)

    barrier = pltpu.get_barrier_semaphore()
    for c in loads[:5]:
        c.start()
    plane = far_first(itertools.product(range(4), range(4), [0], [0]))
    line = far_first(itertools.product([0], [0], range(4), range(2)))
    for o in plane + line:
        pl.semaphore_signal(barrier, inc=1, device_id=device(o), device_id_type=MESH)
    for c in loads[5:]:
        c.start()
    for c in loads[:5]:
        c.wait()
    with jax.named_scope("barrier"):
        pl.semaphore_wait(barrier, kv_n - 1 + tp_n - 1)

    def hand_on(first, count):
        rows = pl.ds(pl.multiple_of((kv * tp_n + first) * 16, 16), count * 16)
        for o in plane:
            send(xall.at[rows], xall.at[rows], st, rt, device(o))

    own_rows = pl.ds(pl.multiple_of(own * 16, 16), 16)
    stage_a = {}
    with jax.named_scope("issue_t"):
        for b, o in enumerate(line):
            _, t = device(o)
            stage_a[o[2:]] = send(xt_ref.at[t // 2, :, lanes_of(t)], xall.at[own_rows], sa.at[b], ra.at[b], (kv, t))
        xall[own_rows, :] = xt_ref[tp // 2, :, lanes_of(tp)]
        own_tile = xt_ref.at[tp // 2, :, lanes_of(tp)]
        for o in plane:
            send(own_tile, xall.at[own_rows], st, rt, device(o))

    for d in (2, 1, 3):
        target = (kv, along_chips(d))
        send(wv_ref, wvz.at[core, chip, 0], sv.at[0], rv.at[0], target)
        send(wz_ref, wvz.at[core, chip, 1], sv.at[1], rv.at[1], target)
    stage_w = [total(wvz.at[core, 0:3, n], sv.at[n], rv.at[n]) for n in range(2)]
    wvz[core, chip, 0] = wv_ref[...]
    wvz[core, chip, 1] = wz_ref[...]
    for o in plane:
        k, _ = device(o)
        cols = pl.ds(pl.multiple_of(k * 128, 128), 128)
        send(wo_ref.at[:, cols], woall.at[chip, kv, core], so, ro, (k, tp))
    woall[chip, kv, core] = wo_ref[:, pl.ds(pl.multiple_of(kv * 128, 128), 128)]
    loads[18].wait()
    for n in range(16):
        column = row_to_column(gain_ref[n : n + 1, :].astype(F32))
        gaincol[n * 128 : n * 128 + 128, :] = jnp.broadcast_to(column, (128, 128))
    hgcol[core] = jnp.broadcast_to(row_to_column(hgain_ref[...].astype(F32)), (16, 128))
    with jax.named_scope("wait_a"):
        stage_a[0, 1].wait_recv()
        hand_on(mate, 1)
        for d in (1, 3, 2):
            for c in range(2):
                stage_a[d, c].wait_recv()
            hand_on(lax.rem(chip + 4 - d, 4) * 2, 2)
    tokens = total(xall.at[0:1920], st, rt)
    for c in loads[5:18]:
        c.wait()

    saves = []

    def store(g, value):
        rows = slice(g * 512, g * 512 + 512)
        accv[rows, :] = value
        abf[g * 512 : g * 512 + 512, :] = value.astype(BF16)

    with jax.named_scope("old"):
        old_part(
            lambda g: state_ref[g * 512 : g * 512 + 512, :],
            lambda g: keys_ref[g * 128 : g * 128 + 128, :],
            [oldv_ref[j].astype(F32) for j in range(4)],
            [logd_ref[j] for j in range(4)],
            [strength_ref[j] for j in range(4)],
            accepted_ref[...],
            store,
        )

    saves.append(pltpu.make_async_copy(accv, acc_ref, acc_sem))
    saves[-1].start()
    out_tiles = total(xall.at[0:240], so, ro)
    out_tiles.wait_recv()
    block = woall.at[chip, :, core]
    for d in (2, 1, 3):
        send(block, block, som.at[1], rom.at[1], (kv, along_chips(d)))
    stage_o = [total(woall.at[0:3, :, core], som.at[1], rom.at[1])]
    theirs = pl.ds(pl.multiple_of((1 - core) * 2048, 2048), 2048)
    to_mate = [send(abf.at[theirs], amate, swm.at[0], rwm.at[0], (kv, mate)), send(hgcol.at[core], hgcol.at[core], swm.at[1], rwm.at[1], (kv, mate))]
    with jax.named_scope("wait_w"):
        for c in stage_w:
            c.wait_recv()
    to_mate.append(send(wvz.at[core], wvz.at[core], swm.at[2], rwm.at[2], (kv, mate)))
    with jax.named_scope("wait_t"):
        tokens.wait_recv()
    with jax.named_scope("project"):
        squares = sum_of([jnp.sum(jnp.square(xall[n * 128 : n * 128 + 128, :].astype(F32)), axis=0, keepdims=True) for n in range(16)])
        scale = lax.rsqrt(squares / 2048.0 + EPS)
        for n in range(16):
            rows = slice(n * 128, n * 128 + 128)
            xnorm[rows, :] = (xall[rows, :].astype(F32) * scale * gaincol[rows, :]).astype(BF16)
        x = xnorm[...]
        qkall[0, chip] = dot(x, wq_ref[...], TN).astype(BF16)
        for d in (2, 1, 3):
            send(qkall.at[0, chip], qkall.at[0, chip], sq.at[0], rq.at[0], (kv, along_chips(d)))
        qkall[1, chip] = dot(x, wk_ref[...], TN).astype(BF16)
        for d in (2, 1, 3):
            send(qkall.at[1, chip], qkall.at[1, chip], sq.at[1], rq.at[1], (kv, along_chips(d)))
        first = iota((16, 2048), 0) == 0
        wsd = jnp.where(first, jnp.broadcast_to(ws_ref[...].astype(F32), (16, 2048)), jnp.broadcast_to(wd_ref[...].astype(F32), (16, 2048)))
        sdall[chip] = dot(wsd.astype(BF16), x)[0:8]
    for d in (2, 1, 3):
        target = (kv, along_chips(d))
        send(sdall.at[chip, pl.ds(0, 2)], sdall.at[chip, pl.ds(0, 2)], sq.at[2], rq.at[2], target)
    stage_c = [total(qkall.at[n, 0:3], sq.at[n], rq.at[n]) for n in range(2)] + [total(sdall.at[0:3, 0:2], sq.at[2], rq.at[2])]
    with jax.named_scope("wait_wm"):
        for c in to_mate:
            c.wait_recv()
    product = dot(wvz[...].reshape(256, 2048), xnorm[...]).astype(BF16).reshape(2, 4, 2, 16, 128)
    for n in range(4):
        for c in range(2):
            vzs[n, c] = product[c, n]
    for d in (2, 1, 3):
        send(vzs.at[lax.rem(chip + d, 4)], vzall.at[chip], svz, rvz, (kv, along_chips(d)))
    stage_v = [total(vzall.at[0:3], svz, rvz)]
    vzall[chip] = vzs[chip]
    with jax.named_scope("wait_c"):
        for c in stage_c:
            c.wait_recv()

    def query_key(m):
        return jnp.concatenate([qkall[n, p, m * 32 : m * 32 + 32, :] for n in range(2) for p in range(4)], axis=0)

    def accepted_state(m):
        return abf[pl.ds(pl.multiple_of((core * 4 + m) * 512, 512), 512), :], amate[m * 512 : m * 512 + 512, :]

    with jax.named_scope("reads"):
        products = new_reads(accepted_state, query_key)
    with jax.named_scope("wait_v"):
        for c in stage_v:
            c.wait_recv()
    with jax.named_scope("new"):
        lanes = pl.ds(pl.multiple_of(core * 128, 128), 128)
        channels = (core, 1 - core)
        outputs = new_part(
            products,
            [[vzall[p, c, 0].astype(F32) for p in range(4)] for c in channels],
            [sdall[p, 0:1, :] for p in range(4)],
            [sdall[p, 1:2, :] for p in range(4)],
            rate_ref[...],
            [prop_ref[j, :, lanes] for j in range(4)],
            [parent_ref[j : j + 1, lanes] for j in range(4)],
        )
        for p in range(4):
            sqs[p] = sum_of([jnp.sum(jnp.square(o[p]), axis=0, keepdims=True) for o in outputs])
            for c, o in zip(channels, outputs):
                z = vzall[p, c, 1].astype(F32)
                ybuf[p, c] = (o[p] * hgcol[c] * (z * jax.nn.sigmoid(z))).astype(BF16)
        place = kv * 4 + chip
        same_core = far_first(itertools.product(range(4), range(4), range(4), [0]))
        for o in same_core:
            k, t = device(o)
            send(ybuf.at[t // 2], yall.at[chip, kv], se, re, (k, t))
        for o in same_core:
            k, t = device(o)
            send(sqs.at[t // 2], sqall.at[place], ses, res, (k, t))
    sqall[place] = sqs[chip]
    yall[chip, kv] = ybuf[chip]
    with jax.named_scope("wait_o"):
        for c in stage_o:
            c.wait_recv()
        block = woall.at[:, :, core]
        stage_o.append(send(block, block, som.at[0], rom.at[0], (kv, mate)))
        stage_o[1].wait_recv()
    with jax.named_scope("wait_e"):
        all_y, all_sq = total(xall.at[0:2016], se, re), total(sqall.at[0:63], ses, res)
        all_sq.wait_recv()
        all_y.wait_recv()
    with jax.named_scope("combine"):
        for k in range(16):
            scale = lax.rsqrt(sum_of([sqall[k * 4 + n] for n in range(4)]) / 128.0 + EPS)
            for c in range(2):
                for n in range(4):
                    rows = slice(((n * 16 + k) * 2 + c) * 16, ((n * 16 + k) * 2 + c) * 16 + 16)
                    ynorm[rows, :] = (yall[n, k, c].astype(F32) * scale).astype(BF16)
        combined = dot(woall[...].reshape(2048, 128), ynorm[...], TN)
        csend[...] = combined.reshape(8, 16, 128)
        sqf[...] = jnp.sum(jnp.square(combined), axis=0, keepdims=True)
    for o in everyone:
        send(sqf, sums_ref.at[tp * 16 + kv], sh, rh, device(o))
    for b, o in enumerate(line):
        _, t = device(o)
        send(csend.at[t], comb_ref.at[tp], sf, rf, (kv, t))
    saves.append(pltpu.make_async_copy(sqf, sums_ref.at[tp * 16 + kv], load_sems.at[0]))
    saves.append(pltpu.make_async_copy(csend.at[tp], comb_ref.at[tp], load_sems.at[1]))
    for c in saves[-2:]:
        c.start()
    stage_f = [total(comb_ref.at[0:7], sf, rf)]
    sums = total(sums_ref.at[0:127], sh, rh)
    with jax.named_scope("sends"):
        for c in list(stage_a.values()) + stage_w + stage_c + stage_v + stage_o + to_mate + [tokens, out_tiles, all_y, all_sq]:
            c.wait_send()
        for c in saves:
            c.wait()
    with jax.named_scope("wait_f"):
        for c in stage_f:
            c.wait_recv()
    with jax.named_scope("wait_h"):
        sums.wait_recv()
    for c in stage_f + [sums]:
        c.wait_send()


def finish(sums_in, comb_in, gain_in, acc_in, out_ref, acc_ref, sums, comb, gain, outv, accv, loaded, saved):
    pieces = [(sums_in, sums), (comb_in, comb), (gain_in, gain)]
    blocks = [pl.ds(g * 512, 512) for g in range(8)]
    pieces += [(acc_in.at[rows], accv.at[rows]) for rows in blocks]
    loads = [pltpu.make_async_copy(a, b, loaded.at[n]) for n, (a, b) in enumerate(pieces)]
    saves = [pltpu.make_async_copy(accv.at[rows], acc_ref.at[rows], saved.at[g]) for g, rows in enumerate(blocks)]
    saves.append(pltpu.make_async_copy(outv, out_ref, saved.at[8]))
    for c in loads:
        c.start()
    for c in loads[:3]:
        c.wait()
    column = jnp.broadcast_to(row_to_column(gain[...].astype(F32)), (16, 128))
    for t in range(8):
        scale = lax.rsqrt(sum_of([sums[t * 16 + k] for k in range(16)]) / 2048.0 + EPS)
        outv[t // 2, :, (t % 2) * 128 : (t % 2) * 128 + 128] = (comb[t] * scale * column).astype(BF16)
    saves[8].start()
    for load, save in zip(loads[3:], saves):
        load.wait()
        save.start()
    for c in saves:
        c.wait()


def on_device(
    tokens, input_norm_gain, query_weight, key_weight, value_weight, output_gate_weight, strength_weight, decay_weight,
    head_decay_rate, proposal_log_decay, head_norm_gain, output_weight, output_norm_gain, state, previous_keys,
    previous_values, previous_log_decay, previous_strengths, accepted, parent,
):
    tp_n, kv_n = lax.axis_size("tp"), lax.axis_size("kv")
    args = [
        tokens.transpose(1, 2, 0),
        value_weight.transpose(1, 2, 0).reshape(16, 2048),
        output_gate_weight.transpose(1, 2, 0).reshape(16, 2048),
        output_weight.reshape(16, 2048),
        input_norm_gain.reshape(16, 128),
        previous_keys.reshape(1024, 128),
        state.reshape(4096, 128),
        previous_values.transpose(1, 2, 3, 0).reshape(4, 16, 256),
        previous_log_decay.transpose(1, 2, 0),
        previous_strengths.transpose(1, 2, 0),
        accepted.reshape(1, 256),
        query_weight,
        key_weight,
        strength_weight.transpose(1, 0),
        decay_weight.transpose(1, 0),
        head_decay_rate.reshape(1, 1),
        proposal_log_decay.transpose(1, 2, 0),
        parent.transpose(1, 0),
        head_norm_gain.reshape(1, 16),
    ]
    hbm = pl.BlockSpec(memory_space=pltpu.HBM)
    specs = [hbm] * len(args)

    def sems(n):
        return [pltpu.SemaphoreType.DMA((n,)), pltpu.SemaphoreType.DMA((n,))]

    def one():
        return [pltpu.SemaphoreType.DMA(()), pltpu.SemaphoreType.DMA(())]

    sums, combined, acc = pl.pallas_call(
        functools.partial(kernel, tp_n, kv_n),
        out_shape=(
            jax.ShapeDtypeStruct((128, 1, 128), F32),
            jax.ShapeDtypeStruct((8, 16, 128), F32),
            jax.ShapeDtypeStruct((4096, 128), F32),
        ),
        in_specs=specs,
        out_specs=(hbm, hbm, hbm),
        scratch_shapes=[
            *[pltpu.VMEM(a.shape, a.dtype) for a in args],
            pltpu.SemaphoreType.DMA((len(args),)),
            pltpu.VMEM((4096, 128), F32),
            pltpu.SemaphoreType.DMA(()),
            pltpu.VMEM((2048, 128), BF16),
            pltpu.VMEM((2, 4, 2, 16, 2048), BF16),
            pltpu.VMEM((4, 16, 2, 16, 128), BF16),
            pltpu.VMEM((2048, 128), F32),
            pltpu.VMEM((2, 16, 128), F32),
            pltpu.VMEM((2048, 128), BF16),
            pltpu.VMEM((2048, 128), BF16),
            pltpu.VMEM((2, 4, 128, 128), BF16),
            pltpu.VMEM((4, 2, 2, 16, 128), BF16),
            pltpu.VMEM((4, 2, 2, 16, 128), BF16),
            pltpu.VMEM((4, 8, 128), F32),
            pltpu.VMEM((4096, 128), BF16),
            pltpu.VMEM((2048, 128), BF16),
            pltpu.VMEM((4, 2, 16, 128), BF16),
            pltpu.VMEM((4, 16, 2, 16, 128), BF16),
            pltpu.VMEM((4, 1, 128), F32),
            pltpu.VMEM((64, 1, 128), F32),
            pltpu.VMEM((8, 16, 128), F32),
            pltpu.VMEM((1, 128), F32),
            *sems(8), *one(), *sems(2), *sems(3), *sems(3), *one(), *one(), *sems(2), *one(), *one(), *one(), *one(),
        ],
        compiler_params=pltpu.CompilerParams(collective_id=0, has_side_effects=True, vmem_limit_bytes=67043328),
    )(*args)
    out, acc = pl.pallas_call(
        finish,
        out_shape=(jax.ShapeDtypeStruct((4, 16, 256), BF16), jax.ShapeDtypeStruct((4096, 128), F32)),
        in_specs=(hbm,) * 4,
        out_specs=(hbm, hbm),
        scratch_shapes=[
            pltpu.VMEM((128, 1, 128), F32),
            pltpu.VMEM((8, 16, 128), F32),
            pltpu.VMEM((1, 16), BF16),
            pltpu.VMEM((4, 16, 256), BF16),
            pltpu.VMEM((4096, 128), F32),
            pltpu.SemaphoreType.DMA((11,)),
            pltpu.SemaphoreType.DMA((9,)),
        ],
        compiler_params=pltpu.CompilerParams(vmem_limit_bytes=67043328),
    )(sums, combined, output_norm_gain.reshape(1, 16), acc)
    return out.transpose(2, 0, 1), acc.reshape(256, 1, 16, 128)


def solution(mesh):
    placed = (
        P(None, None, ("kv", "tp")),
        P(),
        P(None, "kv"),
        P(None, "kv"),
        P(None, "kv", "tp"),
        P(None, "kv", "tp"),
        P(None, "kv"),
        P(None, "kv"),
        P("kv"),
        P(None, None, "kv"),
        P("tp"),
        P("kv", "tp", None),
        P(("kv", "tp")),
        P(None, "kv", "tp", None),
        P(None, None, "kv"),
        P(None, None, "kv", "tp"),
        P(None, None, "kv"),
        P(None, None, "kv"),
        P(),
        P(),
    )
    return jax.shard_map(
        on_device,
        mesh=mesh,
        in_specs=placed,
        out_specs=(P(None, None, ("kv", "tp")), P(None, "kv", "tp", None)),
        check_vma=False,
    )
```

```python
import functools
import itertools

import jax
import jax.numpy as jnp
from jax import lax
from jax.experimental import pallas as pl
from jax.experimental.pallas import tpu as pltpu
from jax.sharding import PartitionSpec as P

EPS = 1e-06
INPUTS = 19
F32 = jnp.float32
BF16 = jnp.bfloat16
MESH = pl.DeviceIdType.MESH
NT = (((1,), (1,)), ((), ()))
NN = (((1,), (0,)), ((), ()))
TN = (((0,), (0,)), ((), ()))


def dot(a, b, dims=NN):
    return lax.dot_general(a, b, dims, preferred_element_type=F32)


def iota(shape, dim):
    return lax.broadcasted_iota(jnp.int32, shape, dim)


def roll(x, shift):
    return x if shift % 128 == 0 else pltpu.roll(x, shift % 128, 1)


def row_to_column(row):
    n = row.shape[1]
    square = jnp.broadcast_to(row, (n, n))
    return jnp.sum(jnp.where(iota((n, n), 0) == iota((n, n), 1), square, 0.0), axis=1, keepdims=True)


def ungroup_half(parts, j):
    chunk = iota(parts[0].shape, 1) // 32
    total = parts[0] if j == 0 else roll(parts[0], -j * 32)
    for m in range(1, 4):
        total = jnp.where(chunk == m, roll(parts[m], (m - j) * 32), total)
    return total


def ungroup(parts, j):
    return jnp.concatenate([ungroup_half(parts[:4], j), ungroup_half(parts[4:], j)], axis=1)


def regroup(rows, g):
    h, m = divmod(g, 4)
    total = None
    for j in range(4):
        x = roll(rows[j][:, h * 128 : h * 128 + 128], (j - m) * 32)
        total = x if total is None else jnp.where(iota(x.shape, 1) // 32 == j, x, total)
    return total


def pick_rows(product):
    lanes = product.shape[1]
    cube = product.reshape(32, 16, lanes)
    keep = iota(cube.shape, 0) == iota(cube.shape, 2) % 32
    return jnp.sum(jnp.where(keep, cube, 0.0), axis=0)


def pick_pairs(product):
    n, lanes = product.shape[0] // 32, product.shape[1]
    cube = product.reshape(n, 32, lanes)
    keep = iota(cube.shape, 1) == iota(cube.shape, 2) % 32
    return jnp.sum(jnp.where(keep, cube, 0.0), axis=1)


def sum_of(terms):
    return functools.reduce(lambda a, b: a + b, terms)


def far_first(offsets):
    return sorted([o for o in offsets if any(o)], key=lambda o: -sum(min(d, 4 - d) for d in o[:3]))


def old_part(state, keys, old_values, log_decay, strengths, accepted, store):
    source, target = iota((128, 128), 1), iota((128, 128), 0)
    order = (source == (target % 32) * 4 + target // 32).astype(BF16)
    grouped, reads, grams = [], [], []
    for g in range(8):
        kg = dot(order, keys(g)).astype(BF16)
        grouped.append(kg)
        reads.append(pick_rows(dot(state(g).astype(BF16), kg, NT)))
        grams.append(pick_pairs(dot(kg, kg, NT)))
    gram = [ungroup(grams, j) for j in range(4)]
    read = [ungroup(reads, j) for j in range(4)]
    inv = [lax.rsqrt(gram[j][j : j + 1] + EPS) for j in range(4)]
    gam, beta = [], []
    for j in range(4):
        live = (j < accepted).astype(F32)
        g_j = log_decay[j] * live
        gam.append(g_j if j == 0 else gam[-1] + g_j)
        beta.append(strengths[j] * live)
    update = []
    for i in range(4):
        u = beta[i] * (old_values[i] - (jnp.exp(gam[i]) * inv[i]) * read[i])
        for j in range(i):
            a = beta[i] * (gram[j][i : i + 1] * (inv[i] * inv[j])) * jnp.exp(gam[i] - gam[j])
            u = u - a * update[j]
        update.append(u)
    weighted = [update[j] * (jnp.exp(gam[3] - gam[j]) * inv[j]) for j in range(4)]
    kept = jnp.exp(gam[3])
    columns = [jnp.broadcast_to(row_to_column(kept[:, h * 128 : h * 128 + 128]), (128, 128)) for h in range(2)]
    for g in range(8):
        wg = regroup(weighted, g)
        cube = (32, 16, 128)
        keep = iota(cube, 0) == iota(cube, 2) % 32
        block = jnp.where(keep, jnp.broadcast_to(wg[None], cube), 0.0).reshape(512, 128).astype(BF16)
        h, m = divmod(g, 4)
        scale = jnp.broadcast_to(columns[h][m * 32 : m * 32 + 32][:, None, :], cube).reshape(512, 128)
        store(g, scale * state(g) + dot(block, grouped[g]))


def new_reads(accepted_state, query_key):
    reads, grams = ([], []), []
    for m in range(4):
        qk = query_key(m)
        for c, state in enumerate(accepted_state(m)):
            reads[c].append(pick_rows(dot(state, qk, NT)))
        grams.append(pick_pairs(dot(qk, qk, NT)))
    aq = [[ungroup_half([r[:, :128] for r in reads[c]], j) for j in range(4)] for c in range(2)]
    ak = [[ungroup_half([r[:, 128:] for r in reads[c]], j) for j in range(4)] for c in range(2)]
    gq = [ungroup_half([r[:, :128] for r in grams], j) for j in range(4)]
    gk = [ungroup_half([r[:, 128:] for r in grams], j) for j in range(4)]
    inv_q = [lax.rsqrt(gq[j][j : j + 1] + EPS) * (128.0**-0.5) for j in range(4)]
    inv_k = [lax.rsqrt(gk[j][4 + j : 5 + j] + EPS) for j in range(4)]
    return aq, ak, gk, inv_q, inv_k


def new_part(products, values, beta_pre, decay_pre, rate, proposal, parent):
    aq, ak, gk, inv_q, inv_k = products
    ancestors = []
    for i in range(4):
        row = {j: (parent[i] == j).astype(F32) for j in range(i)}
        row = {j: row[j] + sum_of([jnp.zeros_like(row[j])] + [row[m] * ancestors[m][j] for m in range(j + 1, i)]) for j in range(i)}
        ancestors.append(row)
    beta, g_new, gam = [], [], []
    for i in range(4):
        x = decay_pre[i]
        softplus = jnp.maximum(x, 0.0) + jnp.log1p(jnp.exp(-jnp.abs(x)))
        g_new.append(-rate * softplus + proposal[i])
        beta.append(jax.nn.sigmoid(beta_pre[i]))
        gam.append(sum_of([g_new[i]] + [ancestors[i][j] * g_new[j] for j in range(i)]))
    outputs, update = ([], []), ([], [])
    for i in range(4):
        grow = jnp.exp(gam[i])
        reach = [jnp.exp(jnp.minimum(gam[i] - gam[j], 0.0)) * ancestors[i][j] * inv_k[j] for j in range(i)]
        for c in range(2):
            u = beta[i] * (values[c][i] - (grow * inv_k[i]) * ak[c][i])
            o = (grow * inv_q[i]) * aq[c][i]
            for j in range(i):
                u = u - (beta[i] * inv_k[i] * gk[j][4 + i : 5 + i] * reach[j]) * update[c][j]
                o = o + (inv_q[i] * gk[j][i : i + 1] * reach[j]) * update[c][j]
            update[c].append(u)
            outputs[c].append(o + (inv_q[i] * gk[i][i : i + 1] * inv_k[i]) * u)
    return outputs


def kernel(
    tp_n, kv_n, *refs,
):
    run(tp_n, kv_n, refs[:INPUTS], *refs[INPUTS:])


def run(
    tp_n, kv_n, sources, sums_ref, comb_ref, acc_ref,
    xt_ref, wv_ref, wz_ref, wo_ref, gain_ref, keys_ref, state_ref, oldv_ref, logd_ref, strength_ref, accepted_ref,
    wq_ref, wk_ref, ws_ref, wd_ref, rate_ref, prop_ref, parent_ref, hgain_ref,
    load_sems, accv, acc_sem,
    xall, wvz, woall, gaincol, hgcol, xnorm, ynorm, qkall, vzs, vzall, sdall, abf, amate, ybuf, yall, sqs, sqall, csend, sqf,
    sa, ra, st, rt, sv, rv, swm, rwm, sq, rq, svz, rvz, so, ro, som, rom, se, re, ses, res, sf, rf, sh, rh,
):
    held = (
        xt_ref, wv_ref, wz_ref, wo_ref, gain_ref, keys_ref, state_ref, oldv_ref, logd_ref, strength_ref, accepted_ref,
        wq_ref, wk_ref, ws_ref, wd_ref, rate_ref, prop_ref, parent_ref, hgain_ref,
    )
    loads = [pltpu.make_async_copy(src, dst, load_sems.at[n]) for n, (src, dst) in enumerate(zip(sources, held))]
    kv, tp = lax.axis_index("kv"), lax.axis_index("tp")
    chip, core = tp // 2, lax.rem(tp, 2)
    mate = tp + 1 - 2 * core
    own = kv * tp_n + tp
    everyone = far_first(itertools.product(range(4), range(4), range(4), range(2)))
    high, low = kv // 4, lax.rem(kv, 4)

    def device(offset):
        z, y, x, c = offset
        return lax.rem(high + z, 4) * 4 + lax.rem(low + y, 4), lax.rem(chip + x, 4) * 2 + lax.rem(core + c, 2)

    def send(src, dst, send_sem, recv_sem, target):
        c = remote(src, dst, send_sem, recv_sem, target)
        c.start()
        return c

    def remote(src, dst, send_sem, recv_sem, target):
        return pltpu.make_async_remote_copy(
            src_ref=src, dst_ref=dst, send_sem=send_sem, recv_sem=recv_sem, device_id=target, device_id_type=MESH
        )

    def total(ref, send_sem, recv_sem):
        return remote(ref, ref, send_sem, recv_sem, (kv, mate))

    def along_chips(d):
        return lax.rem(chip + d, 4) * 2 + core

    def lanes_of(t):
        return pl.ds(pl.multiple_of(lax.rem(t, 2) * 128, 128), 128)

    barrier = pltpu.get_barrier_semaphore()
    for c in loads[:5]:
        c.start()
    plane = far_first(itertools.product(range(4), range(4), [0], [0]))
    line = far_first(itertools.product([0], [0], range(4), range(2)))
    for o in plane + line:
        pl.semaphore_signal(barrier, inc=1, device_id=device(o), device_id_type=MESH)
    for c in loads[5:]:
        c.start()
    for c in loads[:5]:
        c.wait()
    with jax.named_scope("barrier"):
        pl.semaphore_wait(barrier, kv_n - 1 + tp_n - 1)

    def hand_on(first, count):
        rows = pl.ds(pl.multiple_of((kv * tp_n + first) * 16, 16), count * 16)
        for o in plane:
            send(xall.at[rows], xall.at[rows], st, rt, device(o))

    own_rows = pl.ds(pl.multiple_of(own * 16, 16), 16)
    with jax.named_scope("issue_t"):
        for o in line:
            _, t = device(o)
            send(xt_ref.at[t // 2, :, lanes_of(t)], xall.at[own_rows], sa.at[o[2]], ra.at[o[2]], (kv, t))
        xall[own_rows, :] = xt_ref[tp // 2, :, lanes_of(tp)]
        own_tile = xt_ref.at[tp // 2, :, lanes_of(tp)]
        for o in plane:
            send(own_tile, xall.at[own_rows], st, rt, device(o))

    for d in (2, 1, 3):
        target = (kv, along_chips(d))
        send(wv_ref, wvz.at[core, chip, 0], sv.at[0], rv.at[0], target)
        send(wz_ref, wvz.at[core, chip, 1], sv.at[1], rv.at[1], target)
    stage_w = [total(wvz.at[core, 0:3, n], sv.at[n], rv.at[n]) for n in range(2)]
    wvz[core, chip, 0] = wv_ref[...]
    wvz[core, chip, 1] = wz_ref[...]
    for o in plane:
        k, _ = device(o)
        cols = pl.ds(pl.multiple_of(k * 128, 128), 128)
        send(wo_ref.at[:, cols], woall.at[chip, kv, core], so, ro, (k, tp))
    woall[chip, kv, core] = wo_ref[:, pl.ds(pl.multiple_of(kv * 128, 128), 128)]
    loads[18].wait()
    for n in range(16):
        column = row_to_column(gain_ref[n : n + 1, :].astype(F32))
        gaincol[n * 128 : n * 128 + 128, :] = jnp.broadcast_to(column, (128, 128))
    hgcol[core] = jnp.broadcast_to(row_to_column(hgain_ref[...].astype(F32)), (16, 128))
    with jax.named_scope("wait_a"):
        stage_a = {d: total(xall.at[0 : 32 if d else 16], sa.at[d], ra.at[d]) for d in range(4)}
        stage_a[0].wait_recv()
        hand_on(mate, 1)
        for d in (1, 3, 2):
            stage_a[d].wait_recv()
            hand_on(lax.rem(chip + 4 - d, 4) * 2, 2)
    tokens = total(xall.at[0:1920], st, rt)
    for c in loads[5:18]:
        c.wait()

    saves = []

    def store(g, value):
        rows = slice(g * 512, g * 512 + 512)
        accv[rows, :] = value
        abf[g * 512 : g * 512 + 512, :] = value.astype(BF16)

    with jax.named_scope("old"):
        old_part(
            lambda g: state_ref[g * 512 : g * 512 + 512, :],
            lambda g: keys_ref[g * 128 : g * 128 + 128, :],
            [oldv_ref[j].astype(F32) for j in range(4)],
            [logd_ref[j] for j in range(4)],
            [strength_ref[j] for j in range(4)],
            accepted_ref[...],
            store,
        )

    saves.append(pltpu.make_async_copy(accv, acc_ref, acc_sem))
    saves[-1].start()
    out_tiles = total(xall.at[0:240], so, ro)
    out_tiles.wait_recv()
    block = woall.at[chip, :, core]
    for d in (2, 1, 3):
        send(block, block, som.at[1], rom.at[1], (kv, along_chips(d)))
    stage_o = [total(woall.at[0:3, :, core], som.at[1], rom.at[1])]
    theirs = pl.ds(pl.multiple_of((1 - core) * 2048, 2048), 2048)
    to_mate = [send(abf.at[theirs], amate, swm.at[0], rwm.at[0], (kv, mate)), send(hgcol.at[core], hgcol.at[core], swm.at[1], rwm.at[1], (kv, mate))]
    with jax.named_scope("wait_w"):
        for c in stage_w:
            c.wait_recv()
    to_mate.append(send(wvz.at[core], wvz.at[core], swm.at[2], rwm.at[2], (kv, mate)))
    with jax.named_scope("wait_t"):
        tokens.wait_recv()
    with jax.named_scope("project"):
        squares = sum_of([jnp.sum(jnp.square(xall[n * 128 : n * 128 + 128, :].astype(F32)), axis=0, keepdims=True) for n in range(16)])
        scale = lax.rsqrt(squares / 2048.0 + EPS)
        for n in range(16):
            rows = slice(n * 128, n * 128 + 128)
            xnorm[rows, :] = (xall[rows, :].astype(F32) * scale * gaincol[rows, :]).astype(BF16)
        x = xnorm[...]
        qkall[0, chip] = dot(x, wq_ref[...], TN).astype(BF16)
        for d in (2, 1, 3):
            send(qkall.at[0, chip], qkall.at[0, chip], sq.at[0], rq.at[0], (kv, along_chips(d)))
        qkall[1, chip] = dot(x, wk_ref[...], TN).astype(BF16)
        for d in (2, 1, 3):
            send(qkall.at[1, chip], qkall.at[1, chip], sq.at[1], rq.at[1], (kv, along_chips(d)))
        first = iota((16, 2048), 0) == 0
        wsd = jnp.where(first, jnp.broadcast_to(ws_ref[...].astype(F32), (16, 2048)), jnp.broadcast_to(wd_ref[...].astype(F32), (16, 2048)))
        sdall[chip] = dot(wsd.astype(BF16), x)[0:8]
    for d in (2, 1, 3):
        target = (kv, along_chips(d))
        send(sdall.at[chip, pl.ds(0, 2)], sdall.at[chip, pl.ds(0, 2)], sq.at[2], rq.at[2], target)
    stage_c = [total(qkall.at[n, 0:3], sq.at[n], rq.at[n]) for n in range(2)] + [total(sdall.at[0:3, 0:2], sq.at[2], rq.at[2])]
    with jax.named_scope("wait_wm"):
        for c in to_mate:
            c.wait_recv()
    product = dot(wvz[...].reshape(256, 2048), xnorm[...]).astype(BF16).reshape(2, 4, 2, 16, 128)
    for n in range(4):
        for c in range(2):
            vzs[n, c] = product[c, n]
    for d in (2, 1, 3):
        send(vzs.at[lax.rem(chip + d, 4)], vzall.at[chip], svz, rvz, (kv, along_chips(d)))
    stage_v = [total(vzall.at[0:3], svz, rvz)]
    vzall[chip] = vzs[chip]
    with jax.named_scope("wait_c"):
        for c in stage_c:
            c.wait_recv()

    def query_key(m):
        return jnp.concatenate([qkall[n, p, m * 32 : m * 32 + 32, :] for n in range(2) for p in range(4)], axis=0)

    def accepted_state(m):
        return abf[pl.ds(pl.multiple_of((core * 4 + m) * 512, 512), 512), :], amate[m * 512 : m * 512 + 512, :]

    with jax.named_scope("reads"):
        products = new_reads(accepted_state, query_key)
    with jax.named_scope("wait_v"):
        for c in stage_v:
            c.wait_recv()
    with jax.named_scope("new"):
        lanes = pl.ds(pl.multiple_of(core * 128, 128), 128)
        channels = (core, 1 - core)
        outputs = new_part(
            products,
            [[vzall[p, c, 0].astype(F32) for p in range(4)] for c in channels],
            [sdall[p, 0:1, :] for p in range(4)],
            [sdall[p, 1:2, :] for p in range(4)],
            rate_ref[...],
            [prop_ref[j, :, lanes] for j in range(4)],
            [parent_ref[j : j + 1, lanes] for j in range(4)],
        )
        for p in range(4):
            sqs[p] = sum_of([jnp.sum(jnp.square(o[p]), axis=0, keepdims=True) for o in outputs])
            for c, o in zip(channels, outputs):
                z = vzall[p, c, 1].astype(F32)
                ybuf[p, c] = (o[p] * hgcol[c] * (z * jax.nn.sigmoid(z))).astype(BF16)
        place = kv * 4 + chip
        same_core = far_first(itertools.product(range(4), range(4), range(4), [0]))
        for o in same_core:
            k, t = device(o)
            send(ybuf.at[t // 2], yall.at[chip, kv], se, re, (k, t))
        for o in same_core:
            k, t = device(o)
            send(sqs.at[t // 2], sqall.at[place], ses, res, (k, t))
    sqall[place] = sqs[chip]
    yall[chip, kv] = ybuf[chip]
    with jax.named_scope("wait_o"):
        for c in stage_o:
            c.wait_recv()
        block = woall.at[:, :, core]
        stage_o.append(send(block, block, som.at[0], rom.at[0], (kv, mate)))
        stage_o[1].wait_recv()
    with jax.named_scope("wait_e"):
        all_y, all_sq = total(xall.at[0:2016], se, re), total(sqall.at[0:63], ses, res)
        all_sq.wait_recv()
        all_y.wait_recv()
    with jax.named_scope("combine"):
        for k in range(16):
            scale = lax.rsqrt(sum_of([sqall[k * 4 + n] for n in range(4)]) / 128.0 + EPS)
            for c in range(2):
                for n in range(4):
                    rows = slice(((n * 16 + k) * 2 + c) * 16, ((n * 16 + k) * 2 + c) * 16 + 16)
                    ynorm[rows, :] = (yall[n, k, c].astype(F32) * scale).astype(BF16)
        combined = dot(woall[...].reshape(2048, 128), ynorm[...], TN)
        csend[...] = combined.reshape(8, 16, 128)
        sqf[...] = jnp.sum(jnp.square(combined), axis=0, keepdims=True)
    for o in everyone:
        send(sqf, sums_ref.at[tp * 16 + kv], sh, rh, device(o))
    for b, o in enumerate(line):
        _, t = device(o)
        send(csend.at[t], comb_ref.at[tp], sf, rf, (kv, t))
    saves.append(pltpu.make_async_copy(sqf, sums_ref.at[tp * 16 + kv], load_sems.at[0]))
    saves.append(pltpu.make_async_copy(csend.at[tp], comb_ref.at[tp], load_sems.at[1]))
    for c in saves[-2:]:
        c.start()
    stage_f = [total(comb_ref.at[0:7], sf, rf)]
    sums = total(sums_ref.at[0:127], sh, rh)
    with jax.named_scope("sends"):
        for c in list(stage_a.values()) + stage_w + stage_c + stage_v + stage_o + to_mate + [tokens, out_tiles, all_y, all_sq]:
            c.wait_send()
        for c in saves:
            c.wait()
    with jax.named_scope("wait_f"):
        for c in stage_f:
            c.wait_recv()
    with jax.named_scope("wait_h"):
        sums.wait_recv()
    for c in stage_f + [sums]:
        c.wait_send()


def finish(sums_in, comb_in, gain_in, acc_in, out_ref, acc_ref, sums, comb, gain, outv, accv, loaded, saved):
    pieces = [(sums_in, sums), (comb_in, comb), (gain_in, gain)]
    blocks = [pl.ds(g * 1024, 1024) for g in range(4)]
    pieces += [(acc_in.at[rows], accv.at[rows]) for rows in blocks]
    loads = [pltpu.make_async_copy(a, b, loaded.at[n]) for n, (a, b) in enumerate(pieces)]
    saves = [pltpu.make_async_copy(accv.at[rows], acc_ref.at[rows], saved.at[0]) for rows in blocks]
    last = pltpu.make_async_copy(outv, out_ref, saved.at[1])
    for c in loads:
        c.start()
    for c in loads[:3]:
        c.wait()
    column = jnp.broadcast_to(row_to_column(gain[...].astype(F32)), (16, 128))
    for t in range(8):
        scale = lax.rsqrt(sum_of([sums[t * 16 + k] for k in range(16)]) / 2048.0 + EPS)
        outv[t // 2, :, (t % 2) * 128 : (t % 2) * 128 + 128] = (comb[t] * scale * column).astype(BF16)
    last.start()
    for load, save in zip(loads[3:], saves):
        load.wait()
        save.start()
    pltpu.make_async_copy(accv, acc_ref, saved.at[0]).wait()
    last.wait()


def on_device(
    tokens, input_norm_gain, query_weight, key_weight, value_weight, output_gate_weight, strength_weight, decay_weight,
    head_decay_rate, proposal_log_decay, head_norm_gain, output_weight, output_norm_gain, state, previous_keys,
    previous_values, previous_log_decay, previous_strengths, accepted, parent,
):
    tp_n, kv_n = lax.axis_size("tp"), lax.axis_size("kv")
    args = [
        tokens.transpose(1, 2, 0),
        value_weight.transpose(1, 2, 0).reshape(16, 2048),
        output_gate_weight.transpose(1, 2, 0).reshape(16, 2048),
        output_weight.reshape(16, 2048),
        input_norm_gain.reshape(16, 128),
        previous_keys.reshape(1024, 128),
        state.reshape(4096, 128),
        previous_values.transpose(1, 2, 3, 0).reshape(4, 16, 256),
        previous_log_decay.transpose(1, 2, 0),
        previous_strengths.transpose(1, 2, 0),
        accepted.reshape(1, 256),
        query_weight,
        key_weight,
        strength_weight.transpose(1, 0),
        decay_weight.transpose(1, 0),
        head_decay_rate.reshape(1, 1),
        proposal_log_decay.transpose(1, 2, 0),
        parent.transpose(1, 0),
        head_norm_gain.reshape(1, 16),
    ]
    hbm = pl.BlockSpec(memory_space=pltpu.HBM)
    specs = [hbm] * len(args)

    def sems(n):
        return [pltpu.SemaphoreType.DMA((n,)), pltpu.SemaphoreType.DMA((n,))]

    def one():
        return [pltpu.SemaphoreType.DMA(()), pltpu.SemaphoreType.DMA(())]

    sums, combined, acc = pl.pallas_call(
        functools.partial(kernel, tp_n, kv_n),
        out_shape=(
            jax.ShapeDtypeStruct((128, 1, 128), F32),
            jax.ShapeDtypeStruct((8, 16, 128), F32),
            jax.ShapeDtypeStruct((4096, 128), F32),
        ),
        in_specs=specs,
        out_specs=(hbm, hbm, hbm),
        scratch_shapes=[
            *[pltpu.VMEM(a.shape, a.dtype) for a in args],
            pltpu.SemaphoreType.DMA((len(args),)),
            pltpu.VMEM((4096, 128), F32),
            pltpu.SemaphoreType.DMA(()),
            pltpu.VMEM((2048, 128), BF16),
            pltpu.VMEM((2, 4, 2, 16, 2048), BF16),
            pltpu.VMEM((4, 16, 2, 16, 128), BF16),
            pltpu.VMEM((2048, 128), F32),
            pltpu.VMEM((2, 16, 128), F32),
            pltpu.VMEM((2048, 128), BF16),
            pltpu.VMEM((2048, 128), BF16),
            pltpu.VMEM((2, 4, 128, 128), BF16),
            pltpu.VMEM((4, 2, 2, 16, 128), BF16),
            pltpu.VMEM((4, 2, 2, 16, 128), BF16),
            pltpu.VMEM((4, 8, 128), F32),
            pltpu.VMEM((4096, 128), BF16),
            pltpu.VMEM((2048, 128), BF16),
            pltpu.VMEM((4, 2, 16, 128), BF16),
            pltpu.VMEM((4, 16, 2, 16, 128), BF16),
            pltpu.VMEM((4, 1, 128), F32),
            pltpu.VMEM((64, 1, 128), F32),
            pltpu.VMEM((8, 16, 128), F32),
            pltpu.VMEM((1, 128), F32),
            *sems(4), *one(), *sems(2), *sems(3), *sems(3), *one(), *one(), *sems(2), *one(), *one(), *one(), *one(),
        ],
        compiler_params=pltpu.CompilerParams(collective_id=0, has_side_effects=True, vmem_limit_bytes=67043328),
    )(*args)
    out, acc = pl.pallas_call(
        finish,
        out_shape=(jax.ShapeDtypeStruct((4, 16, 256), BF16), jax.ShapeDtypeStruct((4096, 128), F32)),
        in_specs=(hbm,) * 4,
        out_specs=(hbm, hbm),
        scratch_shapes=[
            pltpu.VMEM((128, 1, 128), F32),
            pltpu.VMEM((8, 16, 128), F32),
            pltpu.VMEM((1, 16), BF16),
            pltpu.VMEM((4, 16, 256), BF16),
            pltpu.VMEM((4096, 128), F32),
            pltpu.SemaphoreType.DMA((7,)),
            pltpu.SemaphoreType.DMA((2,)),
        ],
        compiler_params=pltpu.CompilerParams(vmem_limit_bytes=67043328),
    )(sums, combined, output_norm_gain.reshape(1, 16), acc)
    return out.transpose(2, 0, 1), acc.reshape(256, 1, 16, 128)


def solution(mesh):
    placed = (
        P(None, None, ("kv", "tp")),
        P(),
        P(None, "kv"),
        P(None, "kv"),
        P(None, "kv", "tp"),
        P(None, "kv", "tp"),
        P(None, "kv"),
        P(None, "kv"),
        P("kv"),
        P(None, None, "kv"),
        P("tp"),
        P("kv", "tp", None),
        P(("kv", "tp")),
        P(None, "kv", "tp", None),
        P(None, None, "kv"),
        P(None, None, "kv", "tp"),
        P(None, None, "kv"),
        P(None, None, "kv"),
        P(),
        P(),
    )
    return jax.shard_map(
        on_device,
        mesh=mesh,
        in_specs=placed,
        out_specs=(P(None, None, ("kv", "tp")), P(None, "kv", "tp", None)),
        check_vma=False,
    )
```
